256 devices in a mesh: grp: 2 (over y), sp: 32 (over z, core), tp: 4 (over x).
Axes of the slice: x: 4, y: 2, z: 16, core: 2. Of those that a mesh axis runs over, the one named last changes fastest.
The devices are a block of a 4x16x16 slice.
Arguments:
- residual_in: bfloat16 [32768, 2048], P(('grp', 'sp', 'tp')), parts along dimension 0, may hold values from -6 to 6
- out_gate: bfloat16 [32768, 1024], P(('grp', 'sp', 'tp')), parts along dimension 0, may hold values from -6 to 6
- in_gate: bfloat16 [32768, 1024], P(('grp', 'sp', 'tp')), parts along dimension 0, may hold values from -6 to 6
- conv_input: bfloat16 [32768, 1024], P(('grp', 'sp', 'tp')), parts along dimension 0, may hold values from -6 to 6
- conv_kernel: bfloat16 [3, 1024], replicated, may hold values from -3.5 to 3.5
- mix_out: bfloat16 [1024, 2048], replicated, may hold values from -0.1875 to 0.1875
- post_mix_gain: float32 [2048], replicated, may hold values from 0.1 to 1.9
- pre_expert_gain: float32 [2048], replicated, may hold values from 0.1 to 1.9
- post_expert_gain: float32 [2048], replicated, may hold values from 0.1 to 1.9
- expert_ids: int32 [32768, 2], P(('grp', 'sp', 'tp')), parts along dimension 0, may hold values from 0 to 31, all different within a row; in each aligned block of 128 rows (0 to 127, 128 to 255, ...) at most 9 rows name the same one
- expert_weights: float32 [32768, 2], P(('grp', 'sp', 'tp')), parts along dimension 0, may hold values from 0.1 to 1
- gate_proj: bfloat16 [32, 2048, 2048], P('sp', None, 'tp'), may hold values from -0.375 to 0.375
- up_proj: bfloat16 [32, 2048, 2048], P('sp', None, 'tp'), may hold values from -0.375 to 0.375
- down_proj: bfloat16 [32, 2048, 2048], P('sp', 'tp'), may hold values from -0.125 to 0.125
Outputs:
- layer_out: bfloat16 [32768, 2048], P(('grp', 'sp', 'tp')), parts along dimension 0
The draws below stay inside these ranges and needn't reach their ends.
There are 2 independent parts, one for each index of `grp`. The reference program is written for one: setup_inputs(seed, part) draws one part's arguments, and reference() takes and returns one part's arrays. A program takes and returns all parts, laid end to end along the dimension named above; an argument that names none is the same for every part. Nothing has to cross between parts.
Inputs may be any that keep to these rules, and one draw needn't show every extreme that they name: `expert_ids`: each row names 2 different experts. Among the 128 rows of one device no expert is named by more than 9 rows, a bound that some block reaches of them.
All inputs are finite; a program needn't handle non-finite values.
Results may differ from the reference program's by a relative error of at most 0.0095.
Values may be sent and summed in bfloat16 or wider, within the bound.
A program may use at most 64 MiB of HBM per device.

```python
import math
import jax
import jax.numpy as jnp
import numpy as np
from jax import lax

D = 2048
CONV_W = 1024
FF = 2048
TAPS = 3
TOP = 2
TOK_DEV = 128
TOKENS = 16384
EXPERTS = 32
CAP = 9
N_SP = 32
N_TP = 4


def steps_of(stream_key, extent, cuts, least, largest):
    factor_of, own = 1.0, jax.random.fold_in(stream_key, 6)
    for position, shards_of in cuts:
        draws = jnp.exp(jax.random.uniform(jax.random.fold_in(own, position), (shards_of,), jnp.float32, least / len(cuts), largest / len(cuts)))
        factor_of = factor_of * jnp.repeat(draws, extent[position] // shards_of).reshape([-1 if axis == position else 1 for axis in range(len(extent))])
    return factor_of


def shared_out(stream_key, own, number, rows, number_of, top, most, lean):
    ranking = jax.random.permutation(stream_key, number_of)
    heavy_load, common = shares(number_of, rows * top, most, lean, True), shares(number_of, rows * top, most, lean, False)
    places = jnp.arange(number_of)

    def named(lengths, offset_by):
        used = int((lengths > 0).sum())
        fixed = max(1, used // 4)
        passed = fixed + (places - fixed + offset_by * (used - fixed)) % max(1, number_of - fixed)
        return jnp.zeros((number_of,), jnp.int32).at[ranking[jnp.where(places < fixed, places, passed)]].set(jnp.asarray(lengths, jnp.int32))

    lengths = jnp.where(number % 4 == 0, named(heavy_load, number // 4), named(common, number - number // 4 - 1))
    mixed = jax.random.permutation(jax.random.fold_in(own, 3), number_of)
    giver, taker = mixed[0:number_of // 2 * 2:2], mixed[1:number_of // 2 * 2:2]
    margin = jnp.minimum(lengths[giver] - 1, most - lengths[taker]) // 2
    margin = jnp.where((giver == ranking[0]) | (taker == ranking[0]) | (lengths[taker] == 0), 0, jnp.maximum(margin, 0))
    passed = jax.random.randint(jax.random.fold_in(own, 4), (number_of // 2,), 0, 1 << 20) % (margin + 1)
    lengths = lengths.at[giver].add(-passed).at[taker].add(passed)
    labels = jnp.searchsorted(jnp.cumsum(lengths), jnp.arange(rows * top), side="right").astype(jnp.int32)
    listing = labels.reshape(top, rows).T
    listing = listing[jax.random.permutation(jax.random.fold_in(own, 1), rows)]
    offset_by = jax.random.randint(jax.random.fold_in(own, 2), (rows, 1), 0, top)
    return jnp.take_along_axis(listing, (jnp.arange(top)[None, :] + offset_by) % top, axis=1)


def shares(amount, total, most, skew, full):
    loads = [(1 << 20) // math.isqrt(grade ** skew) + 1 for grade in range(1, amount + 1)]
    largest = most if full else min(most, max(-(-total // amount), total * loads[0] // sum(loads)))
    least = 1 if total - largest >= amount - 1 else 0
    holding, rest = [largest] + [least] * (amount - 1), total - largest - least * (amount - 1)
    while rest > 0:
        free = [i for i in range(1, amount) if holding[i] < largest] or [i for i in range(1, amount) if holding[i] < most]
        mass, remaining = sum([loads[i] for i in free]), rest
        for i in free:
            extra = min(most - holding[i], max(1, remaining * loads[i] // mass), rest)
            holding[i] = holding[i] + extra
            rest = rest - extra
    return np.array(holding)


def normal_values(key, shape, scale, limit, split=(), kind=jnp.bfloat16):
    loudness = steps_of(key, shape, split, -0.22, 0.18) if split else 1.0
    entries = jax.random.normal(key, shape, jnp.float32) * scale * loudness
    return jnp.minimum(jnp.maximum(entries, -limit), limit).astype(kind)


def setup_inputs(seed: int = 0, part: int = 0) -> dict:
    arg_keys = jax.random.split(jax.random.key(seed), 15)
    part_keys = jax.random.split(jax.random.fold_in(arg_keys[14], part), 15)
    residual_in = normal_values(part_keys[0], (TOKENS, D), 1.0, 6.0, ((0, 128),))
    out_gate = normal_values(part_keys[1], (TOKENS, CONV_W), 1.0, 6.0, ((0, 128),))
    in_gate = normal_values(part_keys[2], (TOKENS, CONV_W), 1.0, 6.0, ((0, 128),))
    conv_input = normal_values(part_keys[3], (TOKENS, CONV_W), 1.0, 6.0, ((0, 128),))
    conv_kernel = normal_values(arg_keys[4], (TAPS, CONV_W), TAPS ** -0.5, 3.5)
    mix_out = normal_values(arg_keys[5], (CONV_W, D), CONV_W ** -0.5, 0.1875)
    post_mix_gain = jnp.clip(1.0 + 0.18 * jax.random.normal(arg_keys[6], (D,), jnp.float32), 0.1, 1.9)
    pre_expert_gain = jnp.clip(1.0 + 0.18 * jax.random.normal(arg_keys[7], (D,), jnp.float32), 0.1, 1.9)
    post_expert_gain = jnp.clip(1.0 + 0.18 * jax.random.normal(arg_keys[8], (D,), jnp.float32), 0.1, 1.9)
    expert_ids_keys = jax.random.split(jax.random.fold_in(part_keys[9], 1), TOKENS // TOK_DEV)
    expert_ids_turns = jax.random.permutation(jax.random.fold_in(part_keys[9], 3), TOKENS // TOK_DEV)
    expert_ids = jax.vmap(lambda own, number: shared_out(jax.random.fold_in(part_keys[9], 2), own, number, TOK_DEV, EXPERTS, TOP, CAP, 0))(expert_ids_keys, expert_ids_turns).reshape((TOKENS, TOP))
    expert_weights = jnp.clip(jnp.exp(math.log(1.0) - 2.3025851 * jax.random.uniform(part_keys[10], (TOKENS, TOP), jnp.float32) ** steps_of(part_keys[10], (TOKENS, TOP), ((0, 128),), -0.2, 0.2)), 0.1, 1.0)
    gate_proj = normal_values(arg_keys[11], (EXPERTS, D, FF), (D // 9) ** -0.5, 0.375, ((0, 32), (2, 4)))
    up_proj = normal_values(arg_keys[12], (EXPERTS, D, FF), (D // 9) ** -0.5, 0.375, ((0, 32), (2, 4)))
    down_proj = normal_values(arg_keys[13], (EXPERTS, FF, D), FF ** -0.5, 0.125, ((0, 32), (1, 4)))
    return dict(residual_in=residual_in, out_gate=out_gate, in_gate=in_gate, conv_input=conv_input, conv_kernel=conv_kernel, mix_out=mix_out, post_mix_gain=post_mix_gain, pre_expert_gain=pre_expert_gain, post_expert_gain=post_expert_gain, expert_ids=expert_ids, expert_weights=expert_weights, gate_proj=gate_proj, up_proj=up_proj, down_proj=down_proj)


def scaled_norm(values, gain):
    return values * lax.rsqrt(lax.optimization_barrier(jnp.mean(values * values, axis=-1, keepdims=True)) + 1e-06) * gain

def slot_of(routes):
    flat = routes.reshape(-1)
    onehot = (flat[:, None] == jnp.arange(EXPERTS, dtype=jnp.int32)[None, :]).astype(jnp.int32)
    before = jnp.cumsum(onehot, axis=0) - onehot
    return lax.optimization_barrier(jnp.sum(before * onehot, axis=1)).astype(jnp.int32)

def run_expert(rows, gate_w, up_w, down_w):
    gate = jnp.dot(rows, gate_w, preferred_element_type=jnp.float32)
    upper = jnp.dot(rows, up_w, preferred_element_type=jnp.float32)
    gate = jnp.minimum(gate, 7.0)
    upper = jnp.clip(upper, -7.0, 7.0)
    act = (gate * jax.nn.sigmoid(1.702 * gate) * (upper + 1.0)).astype(jnp.bfloat16)
    count = rows.shape[0]
    blocks = act.reshape(count, N_TP, FF // N_TP).astype(jnp.float32)
    down_blocks = down_w.reshape(N_TP, FF // N_TP, D).astype(jnp.float32)
    partial_value = jnp.einsum('npf,pfd->pnd', blocks, down_blocks).astype(jnp.bfloat16)
    return lax.optimization_barrier(jnp.sum(partial_value.astype(jnp.float32), axis=0)).astype(jnp.bfloat16)

def reference(residual_in, out_gate, in_gate, conv_input, conv_kernel, mix_out, post_mix_gain, pre_expert_gain, post_expert_gain, expert_ids, expert_weights, gate_proj, up_proj, down_proj):
    inputs = in_gate.astype(jnp.float32) * conv_input.astype(jnp.float32)
    padded = jnp.concatenate([jnp.zeros((2, CONV_W), jnp.float32), inputs], axis=0)
    taps = conv_kernel.astype(jnp.float32)
    conv = taps[0] * padded[:-2] + taps[1] * padded[1:-1] + taps[2] * padded[2:]
    mixed = (out_gate.astype(jnp.float32) * conv).astype(jnp.bfloat16)
    proj = jnp.dot(mixed, mix_out, preferred_element_type=jnp.float32)
    stream = (residual_in.astype(jnp.float32) + scaled_norm(proj, post_mix_gain)).astype(jnp.bfloat16)
    normed = scaled_norm(stream.astype(jnp.float32), pre_expert_gain).astype(jnp.bfloat16)
    sources = N_SP * N_TP
    routes = expert_ids.reshape(sources, TOK_DEV, TOP)
    slots = jax.vmap(slot_of)(routes)
    flat_e = routes.reshape(sources, TOK_DEV * TOP)
    source_ids = jnp.broadcast_to(jnp.arange(sources, dtype=jnp.int32)[:, None], flat_e.shape)
    token_ids = source_ids * TOK_DEV + (jnp.arange(TOK_DEV * TOP, dtype=jnp.int32) // TOP)[None, :]
    table = jnp.full((EXPERTS, sources, CAP), TOKENS, jnp.int32).at[flat_e, source_ids, slots].set(token_ids)
    weight_table = jnp.zeros((EXPERTS, sources, CAP), jnp.float32).at[flat_e, source_ids, slots].set(expert_weights.reshape(sources, TOK_DEV * TOP))
    padded_rows = jnp.concatenate([normed, jnp.zeros((1, D), jnp.bfloat16)], axis=0)

    def per_expert(total, item):
        index_rows, weight_rows, gate_w, up_w, down_w = item
        flat_index = index_rows.reshape(-1)
        output = run_expert(padded_rows[flat_index], gate_w, up_w, down_w)
        total = total.at[flat_index].add(output.astype(jnp.float32) * weight_rows.reshape(-1)[:, None])
        return (total, None)
    start = jnp.zeros((TOKENS + 1, D), jnp.float32)
    total, unused = lax.scan(per_expert, start, (table, weight_table, gate_proj, up_proj, down_proj))
    moe = total[:TOKENS]
    return (stream.astype(jnp.float32) + scaled_norm(moe, post_expert_gain)).astype(jnp.bfloat16)
```

```python
import functools

import jax
import jax.numpy as jnp
from jax import lax
from jax.experimental import pallas as pl
from jax.experimental.pallas import tpu as pltpu
from jax.sharding import PartitionSpec as P

TOKENS_OVER = ("grp", "sp", "tp")
MESH = pl.DeviceIdType.MESH
F32 = jnp.float32
BF16 = jnp.bfloat16
LANES = 128
ROWS = 8
EPS = 1e-06


def dot(a, b):
    return jnp.dot(a, b, preferred_element_type=F32)


def layer_kernel(
    n_sp,
    n_tp,
    ids_ref,
    wts_ref,
    taps_ref,
    post_mix_ref,
    pre_exp_ref,
    post_exp_ref,
    in_gate_hbm,
    conv_in_hbm,
    out_gate_hbm,
    resid_hbm,
    mix_hbm,
    gate_hbm,
    up_hbm,
    down_hbm,
    out_ref,
    in_gate,
    conv_in,
    out_gate,
    resid,
    mix_w,
    gate_w,
    up_w,
    down_w,
    halo_g,
    halo_c,
    mixed,
    wide,
    stream,
    normed,
    pick,
    outbox,
    rows_in,
    parts_out,
    relay_a,
    relay_b,
    from_left,
    from_right,
    summed,
    returned,
    tail,
    x_rows,
    act,
    r_rows,
    r_last,
    load_sem,
    halo_send,
    halo_recv,
    z_send,
    z_recv,
    g_send,
    g_recv,
    f_send,
    f_recv,
    p_send,
    p_recv,
    d_send,
    d_recv,
    s_send,
    s_recv,
    b_send,
    b_recv,
):
    tokens, width = resid.shape
    conv_w = in_gate.shape[1]
    hidden = gate_w.shape[1]
    chunks = width // LANES
    n_z = n_sp // 2
    steps = n_z // 2
    n_main = n_sp * ROWS
    n_rows = n_main + n_sp
    me = lax.axis_index("sp")
    z, core = me // 2, me % 2
    x = lax.axis_index("tp")
    right = (x + 1) % n_tp
    left = (x + n_tp - 1) % n_tp
    place = me * n_tp + x
    after = (place + 1) % (n_sp * n_tp)
    before = (place + n_sp * n_tp - 1) % (n_sp * n_tp)

    def device_at(p):
        return {"sp": p // n_tp, "tp": p % n_tp}

    bar = pltpu.get_barrier_semaphore()

    def greet(d, carry):
        pl.semaphore_signal(bar, inc=1, device_id={"sp": (me + d) % n_sp}, device_id_type=MESH)
        return carry

    lax.fori_loop(1, n_sp, greet, 0)
    for who in ({"tp": right}, {"tp": left}, device_at(after), device_at(before)):
        pl.semaphore_signal(bar, inc=1, device_id=who, device_id_type=MESH)

    loads = [
        pltpu.make_async_copy(src, dst, load_sem.at[k])
        for k, (src, dst) in enumerate(
            (
                (in_gate_hbm, in_gate),
                (conv_in_hbm, conv_in),
                (out_gate_hbm, out_gate),
                (mix_hbm, mix_w),
                (resid_hbm, resid),
                (gate_hbm, gate_w),
                (up_hbm, up_w),
                (down_hbm, down_w),
            )
        )
    ]
    for load in loads:
        load.start()

    ids = ids_ref[...]
    e_z, e_core = ids // 2, ids % 2
    dz = (e_z - z + n_z) % n_z
    far = dz >= steps
    step_of = jnp.where(far, dz - steps, (steps - dz) % steps)
    message = step_of * 4 + jnp.where(far, 2, 0) + (e_core + core) % 2
    place_iota = lax.broadcasted_iota(jnp.int32, (n_sp, tokens), 0)
    hot = [(place_iota == message[k : k + 1, :]) for k in range(2)]
    both = hot[0].astype(F32) + hot[1].astype(F32)
    earlier = (
        lax.broadcasted_iota(jnp.int32, (tokens, tokens), 0)
        < lax.broadcasted_iota(jnp.int32, (tokens, tokens), 1)
    ).astype(F32)
    count = dot(both.astype(BF16), earlier.astype(BF16))
    row_iota = lax.broadcasted_iota(jnp.int32, (n_rows, tokens), 0)
    gather = []
    for k in range(2):
        slot = jnp.sum(jnp.where(hot[k], count, 0.0), axis=0, keepdims=True).astype(jnp.int32)
        msg = message[k : k + 1, :]
        code = jnp.where(slot < ROWS, msg * ROWS + slot, n_main + msg)
        gather.append((row_iota == code).astype(F32))
    spread = (gather[0] + gather[1]).astype(BF16)

    pl.semaphore_wait(bar, n_sp - 1 + 4)

    halo_rows = halo_g.shape[0]
    halos = []
    for k, (src, dst) in enumerate(((in_gate, halo_g), (conv_in, halo_c))):
        halos.append(
            pltpu.make_async_remote_copy(
                src_ref=src.at[pl.ds(tokens - halo_rows, halo_rows)],
                dst_ref=dst,
                send_sem=halo_send.at[k],
                recv_sem=halo_recv.at[k],
                device_id=device_at(after),
                device_id_type=MESH,
            )
        )
        loads[k].wait()
        halos[k].start()
    loads[2].wait()
    for halo in halos:
        halo.wait_recv()

    taps = taps_ref[...].astype(F32)
    starts = (place == 0).astype(F32)
    col = 256
    for c in range(0, conv_w, col):
        cols = slice(c, c + col)
        u = in_gate[:, cols].astype(F32) * conv_in[:, cols].astype(F32)
        head = halo_g[:, cols].astype(F32) * halo_c[:, cols].astype(F32) * (1.0 - starts)
        padded = jnp.concatenate([head, u], axis=0)
        one = pltpu.roll(padded, 1, 0)[halo_rows:]
        two = pltpu.roll(padded, 2, 0)[halo_rows:]
        conv = taps[0:1, cols] * two + taps[1:2, cols] * one + taps[2:3, cols] * u
        mixed[:, cols] = (out_gate[:, cols].astype(F32) * conv).astype(BF16)
    for halo in halos:
        halo.wait_send()

    loads[3].wait()
    loads[4].wait()
    tile = 512
    square = jnp.zeros((tokens, LANES), F32)

    def fold(v):
        total = v[:, :LANES]
        for k in range(LANES, v.shape[1], LANES):
            total = total + v[:, k : k + LANES]
        return total

    for c in range(0, width, tile):
        cols = slice(c, c + tile)
        proj = dot(mixed[...], mix_w[:, cols])
        wide[:, cols] = proj
        square = square + fold(proj * proj)
    scale = lax.rsqrt(jnp.sum(square, axis=1, keepdims=True) * (1.0 / width) + EPS)
    square = jnp.zeros((tokens, LANES), F32)
    for c in range(0, width, tile):
        cols = slice(c, c + tile)
        s = resid[:, cols].astype(F32) + wide[:, cols] * scale * post_mix_ref[:, cols]
        s = s.astype(BF16)
        stream[:, cols] = s
        s = s.astype(F32)
        square = square + fold(s * s)
    scale = lax.rsqrt(jnp.sum(square, axis=1, keepdims=True) * (1.0 / width) + EPS)
    for c in range(0, width, tile):
        cols = slice(c, c + tile)
        normed[:, cols] = (stream[:, cols].astype(F32) * scale * pre_exp_ref[:, cols]).astype(BF16)

    def pack_main(store, rows, c, count_of):
        pair = [
            rows[: count_of * ROWS, k * LANES : (k + 1) * LANES].reshape(count_of, ROWS, LANES)
            for k in range(2)
        ]
        store(c, jnp.concatenate(pair, axis=1).astype(BF16))

    for c in range(0, chunks, 2):
        rows = dot(spread, normed[:, c * LANES : (c + 2) * LANES])

        def store(c, block):
            outbox[:, c * ROWS : (c + 2) * ROWS, :] = block

        pack_main(store, rows, c, n_sp)
        for k in range(2):
            tail[pl.ds(c + k, n_sp, stride=chunks), :] = rows[
                n_main:, k * LANES : (k + 1) * LANES
            ]
    outbox[:, chunks * ROWS :, :] = tail[...].reshape(n_sp, chunks, LANES).astype(BF16)

    def expert_at(m):
        step, half, cc = m // 4, (m // 2) % 2, m % 2
        far_z = (1 - half) * ((steps - step) % steps) + half * (steps + step)
        return {"sp": ((z + far_z) % n_z) * 2 + (core + cc) % 2}

    def source_at(m):
        step, half, cc = m // 4, (m // 2) % 2, m % 2
        far_z = (1 - half) * ((steps - step) % steps) + half * (steps + step)
        return {"sp": ((z + n_z - far_z) % n_z) * 2 + (core + cc) % 2}

    def dispatch(m):
        return pltpu.make_async_remote_copy(
            src_ref=outbox.at[m],
            dst_ref=rows_in.at[0, m],
            send_sem=z_send.at[m],
            recv_sem=z_recv.at[m],
            device_id=expert_at(m),
            device_id_type=MESH,
        )

    def give_back(m):
        return pltpu.make_async_remote_copy(
            src_ref=summed.at[m],
            dst_ref=returned.at[m],
            send_sem=b_send.at[m],
            recv_sem=b_recv.at[m],
            device_id=source_at(m),
            device_id_type=MESH,
        )

    own_in = pltpu.make_async_copy(outbox.at[0], rows_in.at[0, 0], z_recv.at[0])
    own_back = pltpu.make_async_copy(summed.at[0], returned.at[0], b_recv.at[0])

    def send_out(m, carry):
        dispatch(m).start()
        return carry

    lax.fori_loop(1, n_sp, send_out, 0)
    own_in.start()

    def side(to, src, dst, send, recv):
        return pltpu.make_async_remote_copy(
            src_ref=src,
            dst_ref=dst,
            send_sem=send,
            recv_sem=recv,
            device_id={"tp": to},
            device_id_type=MESH,
        )

    def spread_x(t):
        four = pl.ds(4 * t, 4)
        return (
            side(right, rows_in.at[0, four], rows_in.at[1, four], g_send.at[0, t], g_recv.at[0, t]),
            side(left, rows_in.at[0, four], rows_in.at[3, four], g_send.at[1, t], g_recv.at[1, t]),
        )

    def forward_x(t):
        a, b = pl.ds(4 * t, 2), pl.ds(4 * t + 2, 2)
        return (
            side(right, rows_in.at[1, a], rows_in.at[2, a], f_send.at[0, t], f_recv.at[0, t]),
            side(left, rows_in.at[3, b], rows_in.at[2, b], f_send.at[1, t], f_recv.at[1, t]),
        )

    def across(t):
        a, b = pl.ds(4 * t, 2), pl.ds(4 * t + 2, 2)
        return (
            side(right, parts_out.at[2, a], relay_a.at[t], p_send.at[0, t], p_recv.at[0, t]),
            side(left, parts_out.at[2, b], relay_b.at[t], p_send.at[1, t], p_recv.at[1, t]),
        )

    def direct(t):
        a, b = pl.ds(4 * t, 2), pl.ds(4 * t + 2, 2)
        return (
            side(right, parts_out.at[3, b], from_left.at[b], d_send.at[0, t], d_recv.at[0, t]),
            side(left, parts_out.at[1, a], from_right.at[a], d_send.at[1, t], d_recv.at[1, t]),
        )

    def relayed(t):
        a, b = pl.ds(4 * t, 2), pl.ds(4 * t + 2, 2)
        return (
            side(right, parts_out.at[3, a], from_left.at[a], s_send.at[0, t], s_recv.at[0, t]),
            side(left, parts_out.at[1, b], from_right.at[b], s_send.at[1, t], s_recv.at[1, t]),
        )

    for k in range(2):
        padded = jnp.concatenate(
            [gather[k], jnp.zeros((-n_rows % LANES, tokens), F32)], axis=0
        )
        pick[k * tokens : (k + 1) * tokens, :] = padded.T.astype(BF16)[:, :n_rows]

    def arrive(t):
        def landed(j, carry):
            dispatch(4 * t + j).wait_recv()
            return carry

        lax.fori_loop(0, 4, landed, 0)
        for c in spread_x(t):
            c.start()

    def forward(t):
        for c in spread_x(t):
            c.wait_recv()
        for c in forward_x(t):
            c.start()

    m_in = 4 * n_tp
    main_in = m_in * ROWS

    def experts(t):
        for c in forward_x(t):
            c.wait_recv()
        four = pl.ds(4 * t, 4)
        for q in range(n_tp):
            tail[q * 4 * chunks : (q + 1) * 4 * chunks, :] = (
                rows_in[q, four, chunks * ROWS :, :].astype(F32).reshape(4 * chunks, LANES)
            )
        for c in range(0, chunks, 2):
            block = rows_in[:, four, c * ROWS : (c + 2) * ROWS, :].astype(F32)
            block = block.reshape(m_in, 2 * ROWS, LANES)
            for k in range(2):
                main = block[:, k * ROWS : (k + 1) * ROWS, :].reshape(main_in, LANES)
                last = tail[pl.ds(c + k, m_in, stride=chunks), :]
                x_rows[:, (c + k) * LANES : (c + k + 1) * LANES] = jnp.concatenate(
                    [main, last], axis=0
                ).astype(BF16)
        half = 256
        for c in range(0, hidden, half):
            cols = slice(c, c + half)
            gate = dot(x_rows[...], gate_w[:, cols])
            up = dot(x_rows[...], up_w[:, cols])
            gate = jnp.minimum(gate, 7.0)
            up = jnp.clip(up, -7.0, 7.0)
            act[:, cols] = (gate * jax.nn.sigmoid(1.702 * gate) * (up + 1.0)).astype(BF16)
        for c in range(0, chunks, 2):
            rows = dot(act[...], down_w[:, c * LANES : (c + 2) * LANES])

            def store(c, block):
                parts_out[:, four, c * ROWS : (c + 2) * ROWS, :] = block.reshape(
                    n_tp, 4, 2 * ROWS, LANES
                )

            pack_main(store, rows, c, m_in)
            for k in range(2):
                tail[pl.ds(c + k, m_in, stride=chunks), :] = rows[
                    main_in:, k * LANES : (k + 1) * LANES
                ]
        for q in range(n_tp):
            parts_out[q, four, chunks * ROWS :, :] = (
                tail[q * 4 * chunks : (q + 1) * 4 * chunks, :]
                .reshape(4, chunks, LANES)
                .astype(BF16)
            )
        for c in across(t):
            c.start()
        for c in direct(t):
            c.start()

    def add_relay(t):
        a, b = pl.ds(4 * t, 2), pl.ds(4 * t + 2, 2)
        for c in across(t):
            c.wait_recv()
        parts_out[3, a] = (parts_out[3, a].astype(F32) + relay_a[t].astype(F32)).astype(BF16)
        parts_out[1, b] = (parts_out[1, b].astype(F32) + relay_b[t].astype(F32)).astype(BF16)
        for c in relayed(t):
            c.start()

    def finish(t):
        four = pl.ds(4 * t, 4)
        for c in direct(t):
            c.wait_recv()
        for c in relayed(t):
            c.wait_recv()
        total = from_left[four].astype(F32) + from_right[four].astype(F32)
        summed[four] = (total + parts_out[0, four].astype(F32)).astype(BF16)

        def back(j, carry):
            give_back(4 * t + j).start()
            return carry

        @pl.when(t == 0)
        def _():
            own_back.start()

        lax.fori_loop((t == 0).astype(jnp.int32), 4, back, 0)

    stages = (finish, add_relay, experts, forward, arrive)

    def pipeline(s, carry):
        for k, stage in enumerate(stages):
            t = s - (len(stages) - 1 - k)
            if stage is experts:

                @pl.when(t == 0)
                def _():
                    for load in loads[5:]:
                        load.wait()

            @pl.when((t >= 0) & (t < steps))
            def _():
                stage(t)

        return carry

    lax.fori_loop(0, steps + len(stages) - 1, pipeline, 0)

    for t in range(steps):
        for j in range(4):
            give_back(4 * t + j).wait_recv()
        four = slice(4 * t, 4 * t + 4)
        tail[: 4 * chunks, :] = (
            returned[four, chunks * ROWS :, :].astype(F32).reshape(4 * chunks, LANES)
        )
        for c in range(0, chunks, 2):
            block = returned[four, c * ROWS : (c + 2) * ROWS, :].astype(F32)
            for k in range(2):
                main = block[:, k * ROWS : (k + 1) * ROWS, :].reshape(4 * ROWS, LANES)
                cols = slice((c + k) * LANES, (c + k + 1) * LANES)
                r_rows[4 * t * ROWS : 4 * (t + 1) * ROWS, cols] = main.astype(BF16)
                r_last[4 * t : 4 * t + 4, cols] = tail[pl.ds(c + k, 4, stride=chunks), :]
    weights = jnp.concatenate([wts_ref[...], jnp.zeros((LANES - 2, tokens), F32)], axis=0).T
    square = jnp.zeros((tokens, LANES), F32)
    for c in range(0, width, tile):
        cols = slice(c, c + tile)
        two = dot(pick[:, :n_main], r_rows[:, cols]) + dot(
            pick[:, n_main:], r_last[:, cols].astype(BF16)
        )
        moe = two[:tokens] * weights[:, 0:1] + two[tokens:] * weights[:, 1:2]
        wide[:, cols] = moe
        square = square + fold(moe * moe)
    scale = lax.rsqrt(jnp.sum(square, axis=1, keepdims=True) * (1.0 / width) + EPS)
    for c in range(0, width, tile):
        cols = slice(c, c + tile)
        out_ref[:, cols] = (
            stream[:, cols].astype(F32) + wide[:, cols] * scale * post_exp_ref[:, cols]
        ).astype(BF16)

    def drain(m, carry):
        dispatch(m).wait_send()
        give_back(m).wait_send()
        return carry

    lax.fori_loop(1, n_sp, drain, 0)

    def drain_x(t, carry):
        for copies in (spread_x(t), forward_x(t), across(t), direct(t), relayed(t)):
            for c in copies:
                c.wait_send()
        return carry

    lax.fori_loop(0, steps, drain_x, 0)


def layer(
    n_sp,
    n_tp,
    residual_in,
    out_gate,
    in_gate,
    conv_input,
    conv_kernel,
    mix_out,
    post_mix_gain,
    pre_expert_gain,
    post_expert_gain,
    expert_ids,
    expert_weights,
    gate_proj,
    up_proj,
    down_proj,
):
    tokens, width = residual_in.shape
    conv_w = in_gate.shape[1]
    hidden = gate_proj.shape[2]
    chunks = width // LANES
    steps = n_sp // 4
    msg = (ROWS + 1) * chunks
    n_main = n_sp * ROWS
    rows_step = 4 * n_tp * (ROWS + 1)
    vmem = pl.BlockSpec(memory_space=pltpu.VMEM)
    anyspace = pl.BlockSpec(memory_space=pl.ANY)
    dma = pltpu.SemaphoreType.DMA
    scratch = [
        pltpu.VMEM((tokens, conv_w), BF16),
        pltpu.VMEM((tokens, conv_w), BF16),
        pltpu.VMEM((tokens, conv_w), BF16),
        pltpu.VMEM((tokens, width), BF16),
        pltpu.VMEM((conv_w, width), BF16),
        pltpu.VMEM((width, hidden), BF16),
        pltpu.VMEM((width, hidden), BF16),
        pltpu.VMEM((hidden, width), BF16),
        pltpu.VMEM((16, conv_w), BF16),
        pltpu.VMEM((16, conv_w), BF16),
        pltpu.VMEM((tokens, conv_w), BF16),
        pltpu.VMEM((tokens, width), F32),
        pltpu.VMEM((tokens, width), BF16),
        pltpu.VMEM((tokens, width), BF16),
        pltpu.VMEM((2 * tokens, n_main + n_sp), BF16),
        pltpu.VMEM((n_sp, msg, LANES), BF16),
        pltpu.VMEM((n_tp, n_sp, msg, LANES), BF16),
        pltpu.VMEM((n_tp, n_sp, msg, LANES), BF16),
        pltpu.VMEM((steps, 2, msg, LANES), BF16),
        pltpu.VMEM((steps, 2, msg, LANES), BF16),
        pltpu.VMEM((n_sp, msg, LANES), BF16),
        pltpu.VMEM((n_sp, msg, LANES), BF16),
        pltpu.VMEM((n_sp, msg, LANES), BF16),
        pltpu.VMEM((n_sp, msg, LANES), BF16),
        pltpu.VMEM((n_sp * chunks, LANES), F32),
        pltpu.VMEM((rows_step, width), BF16),
        pltpu.VMEM((rows_step, hidden), BF16),
        pltpu.VMEM((n_main, width), BF16),
        pltpu.VMEM((n_sp, width), F32),
        dma((8,)),
        dma((2,)),
        dma((2,)),
        dma((n_sp,)),
        dma((n_sp,)),
    ]
    scratch += [dma((2, steps)) for _ in range(10)]
    scratch += [dma((n_sp,)), dma((n_sp,))]
    return pl.pallas_call(
        functools.partial(layer_kernel, n_sp, n_tp),
        out_shape=jax.ShapeDtypeStruct((tokens, width), BF16),
        in_specs=[vmem] * 6 + [anyspace] * 8,
        out_specs=vmem,
        scratch_shapes=scratch,
        compiler_params=pltpu.CompilerParams(
            collective_id=0, has_side_effects=True, vmem_limit_bytes=62 * 1024 * 1024
        ),
    )(
        expert_ids.T,
        expert_weights.T,
        conv_kernel,
        post_mix_gain.reshape(1, width),
        pre_expert_gain.reshape(1, width),
        post_expert_gain.reshape(1, width),
        in_gate,
        conv_input,
        out_gate,
        residual_in,
        mix_out,
        gate_proj[0],
        up_proj[0],
        down_proj[0],
    )


def solution(mesh):
    tok = P(TOKENS_OVER, None)
    in_specs = (tok, tok, tok, tok, P(), P(), P(), P(), P(), tok, tok)
    in_specs += (P("sp", None, "tp"), P("sp", None, "tp"), P("sp", "tp", None))
    return jax.shard_map(
        functools.partial(layer, mesh.shape["sp"], mesh.shape["tp"]),
        mesh=mesh,
        in_specs=in_specs,
        out_specs=tok,
        check_vma=False,
    )
```

```python
import functools

import jax
import jax.numpy as jnp
from jax import lax
from jax.experimental import pallas as pl
from jax.experimental.pallas import tpu as pltpu
from jax.sharding import PartitionSpec as P

TOKENS_OVER = ("grp", "sp", "tp")
MESH = pl.DeviceIdType.MESH
F32 = jnp.float32
BF16 = jnp.bfloat16
LANES = 128
ROWS = 8
EPS = 1e-06


def dot(a, b):
    return jnp.dot(a, b, preferred_element_type=F32)


def layer_kernel(
    n_sp,
    n_tp,
    ids_ref,
    wts_ref,
    taps_ref,
    post_mix_ref,
    pre_exp_ref,
    post_exp_ref,
    in_gate_hbm,
    conv_in_hbm,
    out_gate_hbm,
    resid_hbm,
    mix_hbm,
    gate_hbm,
    up_hbm,
    down_hbm,
    out_hbm,
    in_gate,
    conv_in,
    out_gate,
    resid,
    mix_w,
    gate_w,
    up_w,
    down_w,
    edge_g,
    edge_c,
    halo_g,
    halo_c,
    mixed,
    wide,
    stream,
    normed,
    pick,
    outbox,
    rows_in,
    parts_out,
    relay,
    sides,
    summed,
    returned,
    tail,
    x_rows,
    act,
    r_rows,
    r_last,
    out_rows,
    load_sem,
    halo_send,
    halo_recv,
    z_recv,
    g_recv,
    f_recv,
    p_recv,
    s_recv,
    b_recv,
    sent,
):
    tokens, width = resid.shape
    conv_w = in_gate.shape[1]
    hidden = gate_w.shape[1]
    chunks = width // LANES
    n_z = n_sp // 2
    steps = n_z // 2
    n_main = n_sp * ROWS
    n_rows = n_main + n_sp
    me = lax.axis_index("sp")
    z, core = me // 2, me % 2
    x = lax.axis_index("tp")
    right = (x + 1) % n_tp
    left = (x + n_tp - 1) % n_tp
    place = me * n_tp + x
    after = (place + 1) % (n_sp * n_tp)
    before = (place + n_sp * n_tp - 1) % (n_sp * n_tp)

    def device_at(p):
        return {"sp": p // n_tp, "tp": p % n_tp}

    bar = pltpu.get_barrier_semaphore()

    def enter(who):
        pl.semaphore_signal(bar, inc=1, device_id=who, device_id_type=MESH)

    def greet(k, carry):
        far_up = steps - (k + 1) // 2
        up = far_up + (k % 2) * (n_z - 2 * far_up)
        for c in range(2):
            enter({"sp": ((z + up) % n_z) * 2 + c})
        return carry

    lax.fori_loop(0, n_z - 1, greet, 0)
    for who in ({"sp": me + 1 - 2 * core}, device_at(after), device_at(before)):
        enter(who)
    for who in ({"tp": right}, {"tp": left}):
        enter(who)

    loads = [
        pltpu.make_async_copy(src, dst, load_sem.at[k])
        for k, (src, dst) in enumerate(
            (
                (in_gate_hbm, in_gate),
                (conv_in_hbm, conv_in),
                (out_gate_hbm, out_gate),
                (mix_hbm, mix_w),
                (resid_hbm, resid),
                (gate_hbm, gate_w),
                (up_hbm, up_w),
                (down_hbm, down_w),
            )
        )
    ]
    for load in loads:
        load.start()

    ids = ids_ref[...]
    e_z, e_core = ids // 2, ids % 2
    dz = (e_z - z + n_z) % n_z
    far = dz >= steps
    step_of = jnp.where(far, dz - steps, (steps - dz) % steps)
    message = step_of * 4 + jnp.where(far, 2, 0) + (e_core + core) % 2
    place_iota = lax.broadcasted_iota(jnp.int32, (n_sp, tokens), 0)
    hot = [(place_iota == message[k : k + 1, :]) for k in range(2)]
    both = hot[0].astype(F32) + hot[1].astype(F32)
    earlier = (
        lax.broadcasted_iota(jnp.int32, (tokens, tokens), 0)
        < lax.broadcasted_iota(jnp.int32, (tokens, tokens), 1)
    ).astype(F32)
    count = dot(both.astype(BF16), earlier.astype(BF16))
    row_iota = lax.broadcasted_iota(jnp.int32, (n_rows, tokens), 0)
    gather = []
    for k in range(2):
        slot = jnp.sum(jnp.where(hot[k], count, 0.0), axis=0, keepdims=True).astype(jnp.int32)
        msg = message[k : k + 1, :]
        code = jnp.where(slot < ROWS, msg * ROWS + slot, n_main + msg)
        gather.append((row_iota == code).astype(F32))
    spread = (gather[0] + gather[1]).astype(BF16)

    for load, src, edge in ((loads[0], in_gate, edge_g), (loads[1], conv_in, edge_c)):
        load.wait()
        edge[...] = src[tokens - 2 :, :]

    pl.semaphore_wait(bar, n_sp - 1 + 4)

    halos = [
        pltpu.make_async_remote_copy(
            src_ref=src,
            dst_ref=dst,
            send_sem=halo_send.at[k],
            recv_sem=halo_recv.at[k],
            device_id=device_at(after),
            device_id_type=MESH,
        )
        for k, (src, dst) in enumerate(((edge_g, halo_g), (edge_c, halo_c)))
    ]
    for halo in halos:
        halo.start()
    for load in loads[2:5]:
        load.wait()
    for halo in halos:
        halo.wait_recv()

    taps = taps_ref[...].astype(F32)
    row_of = lax.broadcasted_iota(jnp.int32, (tokens, 1), 0)
    inside = (place > 0).astype(F32)
    col = 256
    for c in range(0, conv_w, col):
        cols = slice(c, c + col)
        u = in_gate[:, cols].astype(F32) * conv_in[:, cols].astype(F32)
        head = halo_g[:, cols].astype(F32) * halo_c[:, cols].astype(F32) * inside
        one = jnp.where(row_of == 0, head[1:2], pltpu.roll(u, 1, 0))
        two = jnp.where(row_of == 1, head[1:2], pltpu.roll(u, 2, 0))
        two = jnp.where(row_of == 0, head[0:1], two)
        conv = taps[0:1, cols] * two + taps[1:2, cols] * one + taps[2:3, cols] * u
        mixed[:, cols] = (out_gate[:, cols].astype(F32) * conv).astype(BF16)
    tile = 512
    square = jnp.zeros((tokens, LANES), F32)

    def fold(v):
        total = v[:, :LANES]
        for k in range(LANES, v.shape[1], LANES):
            total = total + v[:, k : k + LANES]
        return total

    for c in range(0, width, tile):
        cols = slice(c, c + tile)
        proj = dot(mixed[...], mix_w[:, cols])
        wide[:, cols] = proj
        square = square + fold(proj * proj)
    scale = lax.rsqrt(jnp.sum(square, axis=1, keepdims=True) * (1.0 / width) + EPS)
    square = jnp.zeros((tokens, LANES), F32)
    for c in range(0, width, tile):
        cols = slice(c, c + tile)
        s = resid[:, cols].astype(F32) + wide[:, cols] * scale * post_mix_ref[:, cols]
        s = s.astype(BF16)
        stream[:, cols] = s
        s = s.astype(F32)
        square = square + fold(s * s)
    scale = lax.rsqrt(jnp.sum(square, axis=1, keepdims=True) * (1.0 / width) + EPS)
    for c in range(0, width, tile):
        cols = slice(c, c + tile)
        normed[:, cols] = (stream[:, cols].astype(F32) * scale * pre_exp_ref[:, cols]).astype(BF16)

    def pack_main(store, rows, c, count_of):
        pair = [
            rows[: count_of * ROWS, k * LANES : (k + 1) * LANES].reshape(count_of, ROWS, LANES)
            for k in range(2)
        ]
        store(c, jnp.concatenate(pair, axis=1).astype(BF16))

    for c in range(0, chunks, 2):
        rows = dot(spread, normed[:, c * LANES : (c + 2) * LANES])

        def store(c, block):
            outbox[:, c * ROWS : (c + 2) * ROWS, :] = block

        pack_main(store, rows, c, n_sp)
        for k in range(2):
            tail[pl.ds(c + k, n_sp, stride=chunks), :] = rows[
                n_main:, k * LANES : (k + 1) * LANES
            ]
    outbox[:, chunks * ROWS :, :] = tail[...].reshape(n_sp, chunks, LANES).astype(BF16)

    def expert_at(m):
        step, half, cc = m // 4, (m // 2) % 2, m % 2
        far_z = (1 - half) * ((steps - step) % steps) + half * (steps + step)
        return {"sp": ((z + far_z) % n_z) * 2 + (core + cc) % 2}

    def source_at(m):
        step, half, cc = m // 4, (m // 2) % 2, m % 2
        far_z = (1 - half) * ((steps - step) % steps) + half * (steps + step)
        return {"sp": ((z + n_z - far_z) % n_z) * 2 + (core + cc) % 2}

    def took(ref, sem):
        pltpu.make_async_copy(ref, ref, sem).wait()

    def dispatch(m):
        pltpu.make_async_remote_copy(
            src_ref=outbox.at[m],
            dst_ref=rows_in.at[0, m],
            send_sem=sent.at[0],
            recv_sem=z_recv.at[m // 4],
            device_id=expert_at(m),
            device_id_type=MESH,
        ).start()

    def give_back(m):
        pltpu.make_async_remote_copy(
            src_ref=summed.at[m],
            dst_ref=returned.at[m],
            send_sem=sent.at[1],
            recv_sem=b_recv.at[m // 4],
            device_id=source_at(m),
            device_id_type=MESH,
        ).start()

    def order(t):
        return (t + steps - 1) % steps

    def send_out(k, carry):
        m = (k + n_sp - 4) % n_sp

        @pl.when(m > 0)
        def _():
            dispatch(m)

        return carry

    pltpu.make_async_copy(outbox.at[0], rows_in.at[0, 0], z_recv.at[0]).start()
    lax.fori_loop(0, n_sp, send_out, 0)

    def side(to, src, dst, send, recv):
        pltpu.make_async_remote_copy(
            src_ref=src,
            dst_ref=dst,
            send_sem=sent.at[send],
            recv_sem=recv,
            device_id={"tp": to},
            device_id_type=MESH,
        ).start()

    for k in range(2):
        padded = jnp.concatenate(
            [gather[k], jnp.zeros((-n_rows % LANES, tokens), F32)], axis=0
        )
        pick[k * tokens : (k + 1) * tokens, :] = padded.T.astype(BF16)[:, :n_rows]

    def arrive(t):
        four = pl.ds(4 * t, 4)
        took(rows_in.at[0, four], z_recv.at[t])
        side(right, rows_in.at[0, four], rows_in.at[1, four], 2, g_recv.at[t])
        side(left, rows_in.at[0, four], rows_in.at[3, four], 2, g_recv.at[t])

    def forward(t):
        a, b = pl.ds(4 * t, 2), pl.ds(4 * t + 2, 2)
        took(rows_in.at[pl.ds(0, 2), pl.ds(4 * t, 4)], g_recv.at[t])
        side(right, rows_in.at[1, a], rows_in.at[2, a], 3, f_recv.at[t])
        side(left, rows_in.at[3, b], rows_in.at[2, b], 3, f_recv.at[t])

    m_in = 4 * n_tp
    main_in = m_in * ROWS

    def experts(t):
        four = pl.ds(4 * t, 4)
        took(rows_in.at[2, four], f_recv.at[t])
        for q in range(n_tp):
            tail[q * 4 * chunks : (q + 1) * 4 * chunks, :] = (
                rows_in[q, four, chunks * ROWS :, :].astype(F32).reshape(4 * chunks, LANES)
            )
        for c in range(0, chunks, 2):
            block = rows_in[:, four, c * ROWS : (c + 2) * ROWS, :].astype(F32)
            block = block.reshape(m_in, 2 * ROWS, LANES)
            for k in range(2):
                main = block[:, k * ROWS : (k + 1) * ROWS, :].reshape(main_in, LANES)
                last = tail[pl.ds(c + k, m_in, stride=chunks), :]
                x_rows[:, (c + k) * LANES : (c + k + 1) * LANES] = jnp.concatenate(
                    [main, last], axis=0
                ).astype(BF16)
        half = 256
        for c in range(0, hidden, half):
            cols = slice(c, c + half)
            gate = dot(x_rows[...], gate_w[:, cols])
            up = dot(x_rows[...], up_w[:, cols])
            gate = jnp.minimum(gate, 7.0)
            up = jnp.clip(up, -7.0, 7.0)
            act[:, cols] = (gate * jax.nn.sigmoid(1.702 * gate) * (up + 1.0)).astype(BF16)
        for c in range(0, chunks, 2):
            rows = dot(act[...], down_w[:, c * LANES : (c + 2) * LANES])

            def store(c, block):
                parts_out[:, four, c * ROWS : (c + 2) * ROWS, :] = block.reshape(
                    n_tp, 4, 2 * ROWS, LANES
                )

            pack_main(store, rows, c, m_in)
            for k in range(2):
                tail[pl.ds(c + k, m_in, stride=chunks), :] = rows[
                    main_in:, k * LANES : (k + 1) * LANES
                ]
        for q in range(n_tp):
            parts_out[q, four, chunks * ROWS :, :] = (
                tail[q * 4 * chunks : (q + 1) * 4 * chunks, :]
                .reshape(4, chunks, LANES)
                .astype(BF16)
            )
        a, b = pl.ds(4 * t, 2), pl.ds(4 * t + 2, 2)
        side(right, parts_out.at[2, a], relay.at[t, pl.ds(0, 2)], 4, p_recv.at[t])
        side(left, parts_out.at[2, b], relay.at[t, pl.ds(2, 2)], 4, p_recv.at[t])
        side(right, parts_out.at[3, b], sides.at[0, b], 5, s_recv.at[t])
        side(left, parts_out.at[1, a], sides.at[1, a], 5, s_recv.at[t])

    def add_relay(t):
        a, b = pl.ds(4 * t, 2), pl.ds(4 * t + 2, 2)
        took(relay.at[t], p_recv.at[t])
        parts_out[3, a] = (parts_out[3, a].astype(F32) + relay[t, 0:2].astype(F32)).astype(BF16)
        parts_out[1, b] = (parts_out[1, b].astype(F32) + relay[t, 2:4].astype(F32)).astype(BF16)
        side(right, parts_out.at[3, a], sides.at[0, a], 6, s_recv.at[t])
        side(left, parts_out.at[1, b], sides.at[1, b], 6, s_recv.at[t])

    def finish(t):
        four = pl.ds(4 * t, 4)
        took(sides.at[:, four], s_recv.at[t])
        total = sides[0, four].astype(F32) + sides[1, four].astype(F32)
        summed[four] = (total + parts_out[0, four].astype(F32)).astype(BF16)

        def back(j, carry):
            give_back(4 * t + j)
            return carry

        lax.fori_loop((t == 0).astype(jnp.int32), 4, back, 0)

        @pl.when(t == 0)
        def _():
            pltpu.make_async_copy(summed.at[0], returned.at[0], b_recv.at[0]).start()

    stages = (finish, add_relay, experts, forward, arrive)

    def pipeline(s, carry):
        for k, stage in enumerate(stages):
            t = s - (len(stages) - 1 - k)
            if stage is experts:

                @pl.when(t == 0)
                def _():
                    for load in loads[5:]:
                        load.wait()

            @pl.when((t >= 0) & (t < steps))
            def _():
                stage(order(t))

        return carry

    lax.fori_loop(0, steps + len(stages) - 1, pipeline, 0)

    for k in range(steps):
        t = order(k)
        four = slice(4 * t, 4 * t + 4)
        took(returned.at[pl.ds(4 * t, 4)], b_recv.at[t])
        tail[: 4 * chunks, :] = (
            returned[four, chunks * ROWS :, :].astype(F32).reshape(4 * chunks, LANES)
        )
        for c in range(0, chunks, 2):
            block = returned[four, c * ROWS : (c + 2) * ROWS, :].astype(F32)
            for k in range(2):
                main = block[:, k * ROWS : (k + 1) * ROWS, :].reshape(4 * ROWS, LANES)
                cols = slice((c + k) * LANES, (c + k + 1) * LANES)
                r_rows[4 * t * ROWS : 4 * (t + 1) * ROWS, cols] = main.astype(BF16)
                r_last[4 * t : 4 * t + 4, cols] = tail[pl.ds(c + k, 4, stride=chunks), :]

    def out_copy(c):
        cols = pl.ds(c, tile)
        return pltpu.make_async_copy(out_rows.at[:, cols], out_hbm.at[:, cols], sent.at[7])

    weights = jnp.concatenate([wts_ref[...], jnp.zeros((LANES - 2, tokens), F32)], axis=0).T
    square = jnp.zeros((tokens, LANES), F32)
    for c in range(0, width, tile):
        cols = slice(c, c + tile)
        two = dot(pick[:, :n_main], r_rows[:, cols]) + dot(
            pick[:, n_main:], r_last[:, cols].astype(BF16)
        )
        moe = two[:tokens] * weights[:, 0:1] + two[tokens:] * weights[:, 1:2]
        wide[:, cols] = moe
        square = square + fold(moe * moe)
    scale = lax.rsqrt(jnp.sum(square, axis=1, keepdims=True) * (1.0 / width) + EPS)
    for c in range(0, width, tile):
        cols = slice(c, c + tile)
        out_rows[:, cols] = (
            stream[:, cols].astype(F32) + wide[:, cols] * scale * post_exp_ref[:, cols]
        ).astype(BF16)
        out_copy(c).start()

    for halo in halos:
        halo.wait_send()
    took(outbox.at[pl.ds(1, n_sp - 1)], sent.at[0])
    took(summed.at[pl.ds(1, n_sp - 1)], sent.at[1])
    took(rows_in.at[pl.ds(0, 2)], sent.at[2])
    took(rows_in.at[0], sent.at[3])
    for k in range(4, 7):
        took(parts_out.at[0], sent.at[k])
    took(out_rows, sent.at[7])


def layer(
    n_sp,
    n_tp,
    residual_in,
    out_gate,
    in_gate,
    conv_input,
    conv_kernel,
    mix_out,
    post_mix_gain,
    pre_expert_gain,
    post_expert_gain,
    expert_ids,
    expert_weights,
    gate_proj,
    up_proj,
    down_proj,
):
    tokens, width = residual_in.shape
    conv_w = in_gate.shape[1]
    hidden = gate_proj.shape[2]
    chunks = width // LANES
    steps = n_sp // 4
    msg = (ROWS + 1) * chunks
    n_main = n_sp * ROWS
    rows_step = 4 * n_tp * (ROWS + 1)
    vmem = pl.BlockSpec(memory_space=pltpu.VMEM)
    anyspace = pl.BlockSpec(memory_space=pl.ANY)
    dma = pltpu.SemaphoreType.DMA
    scratch = [
        pltpu.VMEM((tokens, conv_w), BF16),
        pltpu.VMEM((tokens, conv_w), BF16),
        pltpu.VMEM((tokens, conv_w), BF16),
        pltpu.VMEM((tokens, width), BF16),
        pltpu.VMEM((conv_w, width), BF16),
        pltpu.VMEM((width, hidden), BF16),
        pltpu.VMEM((width, hidden), BF16),
        pltpu.VMEM((hidden, width), BF16),
        pltpu.VMEM((2, conv_w), BF16),
        pltpu.VMEM((2, conv_w), BF16),
        pltpu.VMEM((2, conv_w), BF16),
        pltpu.VMEM((2, conv_w), BF16),
        pltpu.VMEM((tokens, conv_w), BF16),
        pltpu.VMEM((tokens, width), F32),
        pltpu.VMEM((tokens, width), BF16),
        pltpu.VMEM((tokens, width), BF16),
        pltpu.VMEM((2 * tokens, n_main + n_sp), BF16),
        pltpu.VMEM((n_sp, msg, LANES), BF16),
        pltpu.VMEM((n_tp, n_sp, msg, LANES), BF16),
        pltpu.VMEM((n_tp, n_sp, msg, LANES), BF16),
        pltpu.VMEM((steps, 4, msg, LANES), BF16),
        pltpu.VMEM((2, n_sp, msg, LANES), BF16),
        pltpu.VMEM((n_sp, msg, LANES), BF16),
        pltpu.VMEM((n_sp, msg, LANES), BF16),
        pltpu.VMEM((n_sp * chunks, LANES), F32),
        pltpu.VMEM((rows_step, width), BF16),
        pltpu.VMEM((rows_step, hidden), BF16),
        pltpu.VMEM((n_main, width), BF16),
        pltpu.VMEM((n_sp, width), F32),
        pltpu.VMEM((tokens, width), BF16),
        dma((8,)),
        dma((2,)),
        dma((2,)),
    ]
    scratch += [dma((steps,)) for _ in range(6)]
    scratch += [dma((8,))]
    return pl.pallas_call(
        functools.partial(layer_kernel, n_sp, n_tp),
        out_shape=jax.ShapeDtypeStruct((tokens, width), BF16),
        in_specs=[vmem] * 6 + [anyspace] * 8,
        out_specs=anyspace,
        scratch_shapes=scratch,
        compiler_params=pltpu.CompilerParams(
            collective_id=0, has_side_effects=True, vmem_limit_bytes=62 * 1024 * 1024
        ),
    )(
        expert_ids.T,
        expert_weights.T,
        conv_kernel,
        post_mix_gain.reshape(1, width),
        pre_expert_gain.reshape(1, width),
        post_expert_gain.reshape(1, width),
        in_gate,
        conv_input,
        out_gate,
        residual_in,
        mix_out,
        gate_proj[0],
        up_proj[0],
        down_proj[0],
    )


def solution(mesh):
    tok = P(TOKENS_OVER, None)
    in_specs = (tok, tok, tok, tok, P(), P(), P(), P(), P(), tok, tok)
    in_specs += (P("sp", None, "tp"), P("sp", None, "tp"), P("sp", "tp", None))
    return jax.shard_map(
        functools.partial(layer, mesh.shape["sp"], mesh.shape["tp"]),
        mesh=mesh,
        in_specs=in_specs,
        out_specs=tok,
        check_vma=False,
    )
```

```python
import functools

import jax
import jax.numpy as jnp
from jax import lax
from jax.experimental import pallas as pl
from jax.experimental.pallas import tpu as pltpu
from jax.sharding import PartitionSpec as P

TOKENS_OVER = ("grp", "sp", "tp")
MESH = pl.DeviceIdType.MESH
F32 = jnp.float32
BF16 = jnp.bfloat16
LANES = 128
ROWS = 8
EPS = 1e-06


def dot(a, b):
    return jnp.dot(a, b, preferred_element_type=F32)


def layer_kernel(
    n_sp,
    n_tp,
    ids_hbm,
    wts_hbm,
    taps_hbm,
    post_mix_hbm,
    pre_exp_hbm,
    post_exp_hbm,
    in_gate_hbm,
    conv_in_hbm,
    out_gate_hbm,
    resid_hbm,
    mix_hbm,
    gate_hbm,
    up_hbm,
    down_hbm,
    out_hbm,
    ids_ref,
    wts_ref,
    taps_ref,
    post_mix_ref,
    pre_exp_ref,
    post_exp_ref,
    in_gate,
    conv_in,
    out_gate,
    resid,
    mix_w,
    gate_w,
    up_w,
    down_w,
    edge_g,
    edge_c,
    halo_g,
    halo_c,
    mixed,
    wide,
    stream,
    normed,
    pick,
    outbox,
    rows_in,
    parts_out,
    relay,
    sides,
    summed,
    returned,
    tail,
    x_rows,
    act,
    r_rows,
    r_last,
    out_rows,
    load_sem,
    halo_send,
    halo_recv,
    z_recv,
    g_recv,
    f_recv,
    p_recv,
    s_recv,
    b_recv,
    sent,
):
    tokens, width = resid.shape
    conv_w = in_gate.shape[1]
    hidden = gate_w.shape[1]
    chunks = width // LANES
    n_z = n_sp // 2
    steps = n_z // 2
    n_main = n_sp * ROWS
    n_rows = n_main + n_sp
    me = lax.axis_index("sp")
    z, core = me // 2, me % 2
    x = lax.axis_index("tp")
    right = (x + 1) % n_tp
    left = (x + n_tp - 1) % n_tp
    place = me * n_tp + x
    after = (place + 1) % (n_sp * n_tp)
    before = (place + n_sp * n_tp - 1) % (n_sp * n_tp)

    def device_at(p):
        return {"sp": p // n_tp, "tp": p % n_tp}

    bar = pltpu.get_barrier_semaphore()

    def enter(who):
        pl.semaphore_signal(bar, inc=1, device_id=who, device_id_type=MESH)

    def greet(k, carry):
        far_up = steps - (k + 1) // 2
        up = far_up + (k % 2) * (n_z - 2 * far_up)
        for c in range(2):
            enter({"sp": ((z + up) % n_z) * 2 + c})
        return carry

    lax.fori_loop(0, n_z - 1, greet, 0)
    for who in ({"sp": me + 1 - 2 * core}, device_at(after), device_at(before)):
        enter(who)
    for who in ({"tp": right}, {"tp": left}):
        enter(who)

    loads = [
        pltpu.make_async_copy(src, dst, load_sem.at[k])
        for k, (src, dst) in enumerate(
            (
                (in_gate_hbm, in_gate),
                (conv_in_hbm, conv_in),
                (out_gate_hbm, out_gate),
                (mix_hbm, mix_w),
                (resid_hbm, resid),
                (gate_hbm, gate_w),
                (up_hbm, up_w),
                (down_hbm, down_w),
                (ids_hbm, ids_ref),
                (taps_hbm, taps_ref),
                (post_mix_hbm, post_mix_ref),
                (pre_exp_hbm, pre_exp_ref),
                (wts_hbm, wts_ref),
                (post_exp_hbm, post_exp_ref),
            )
        )
    ]
    for load in loads[:2] + loads[8:10] + loads[2:5] + loads[10:] + loads[5:8]:
        load.start()
    loads[8].wait()

    ids = ids_ref[...]
    e_z, e_core = ids // 2, ids % 2
    dz = (e_z - z + n_z) % n_z
    far = dz >= steps
    step_of = jnp.where(far, dz - steps, (steps - dz) % steps)
    message = step_of * 4 + jnp.where(far, 2, 0) + (e_core + core) % 2
    place_iota = lax.broadcasted_iota(jnp.int32, (n_sp, tokens), 0)
    hot = [(place_iota == message[k : k + 1, :]) for k in range(2)]
    both = hot[0].astype(F32) + hot[1].astype(F32)
    earlier = (
        lax.broadcasted_iota(jnp.int32, (tokens, tokens), 0)
        < lax.broadcasted_iota(jnp.int32, (tokens, tokens), 1)
    ).astype(F32)
    count = dot(both.astype(BF16), earlier.astype(BF16))
    row_iota = lax.broadcasted_iota(jnp.int32, (n_rows, tokens), 0)
    gather = []
    for k in range(2):
        slot = jnp.sum(jnp.where(hot[k], count, 0.0), axis=0, keepdims=True).astype(jnp.int32)
        msg = message[k : k + 1, :]
        code = jnp.where(slot < ROWS, msg * ROWS + slot, n_main + msg)
        gather.append((row_iota == code).astype(F32))
    spread = (gather[0] + gather[1]).astype(BF16)

    for load, src, edge in ((loads[0], in_gate, edge_g), (loads[1], conv_in, edge_c)):
        load.wait()
        edge[...] = src[tokens - 2 :, :]

    head_rows = 16
    inside = (place > 0).astype(F32)
    loads[9].wait()
    taps = taps_ref[...].astype(F32)

    def convolve(rows, with_halo):
        row_of = lax.broadcasted_iota(jnp.int32, (rows, 1), 0)
        col = 256
        for c in range(0, conv_w, col):
            cols = slice(c, c + col)
            u = in_gate[:rows, cols].astype(F32) * conv_in[:rows, cols].astype(F32)
            one, two = pltpu.roll(u, 1, 0), pltpu.roll(u, 2, 0)
            if with_halo:
                head = halo_g[:, cols].astype(F32) * halo_c[:, cols].astype(F32) * inside
                one = jnp.where(row_of == 0, head[1:2], one)
                two = jnp.where(row_of == 1, head[1:2], two)
                two = jnp.where(row_of == 0, head[0:1], two)
            conv = taps[0:1, cols] * two + taps[1:2, cols] * one + taps[2:3, cols] * u
            mixed[:rows, cols] = (out_gate[:rows, cols].astype(F32) * conv).astype(BF16)

    loads[2].wait()
    convolve(tokens, False)
    pl.semaphore_wait(bar, n_sp - 1 + 4)

    halos = [
        pltpu.make_async_remote_copy(
            src_ref=src,
            dst_ref=dst,
            send_sem=halo_send.at[k],
            recv_sem=halo_recv.at[k],
            device_id=device_at(after),
            device_id_type=MESH,
        )
        for k, (src, dst) in enumerate(((edge_g, halo_g), (edge_c, halo_c)))
    ]
    for halo in halos:
        halo.start()
    for load in loads[3:5] + loads[10:]:
        load.wait()
    for halo in halos:
        halo.wait_recv()
    convolve(head_rows, True)

    tile = 512
    square = jnp.zeros((tokens, LANES), F32)

    def fold(v):
        total = v[:, :LANES]
        for k in range(LANES, v.shape[1], LANES):
            total = total + v[:, k : k + LANES]
        return total

    for c in range(0, width, tile):
        cols = slice(c, c + tile)
        proj = dot(mixed[...], mix_w[:, cols])
        wide[:, cols] = proj
        square = square + fold(proj * proj)
    scale = lax.rsqrt(jnp.sum(square, axis=1, keepdims=True) * (1.0 / width) + EPS)
    square = jnp.zeros((tokens, LANES), F32)
    for c in range(0, width, tile):
        cols = slice(c, c + tile)
        s = resid[:, cols].astype(F32) + wide[:, cols] * scale * post_mix_ref[:, cols]
        s = s.astype(BF16)
        stream[:, cols] = s
        s = s.astype(F32)
        square = square + fold(s * s)
    scale = lax.rsqrt(jnp.sum(square, axis=1, keepdims=True) * (1.0 / width) + EPS)
    for c in range(0, width, tile):
        cols = slice(c, c + tile)
        normed[:, cols] = (stream[:, cols].astype(F32) * scale * pre_exp_ref[:, cols]).astype(BF16)

    def pack_main(store, rows, c, count_of):
        pair = [
            rows[: count_of * ROWS, k * LANES : (k + 1) * LANES].reshape(count_of, ROWS, LANES)
            for k in range(2)
        ]
        store(c, jnp.concatenate(pair, axis=1).astype(BF16))

    for c in range(0, chunks, 2):
        rows = dot(spread, normed[:, c * LANES : (c + 2) * LANES])

        def store(c, block):
            outbox[:, c * ROWS : (c + 2) * ROWS, :] = block

        pack_main(store, rows, c, n_sp)
        for k in range(2):
            tail[pl.ds(c + k, n_sp, stride=chunks), :] = rows[
                n_main:, k * LANES : (k + 1) * LANES
            ]
    outbox[:, chunks * ROWS :, :] = tail[...].reshape(n_sp, chunks, LANES).astype(BF16)

    def expert_at(m):
        step, half, cc = m // 4, (m // 2) % 2, m % 2
        far_z = (1 - half) * ((steps - step) % steps) + half * (steps + step)
        return {"sp": ((z + far_z) % n_z) * 2 + (core + cc) % 2}

    def source_at(m):
        step, half, cc = m // 4, (m // 2) % 2, m % 2
        far_z = (1 - half) * ((steps - step) % steps) + half * (steps + step)
        return {"sp": ((z + n_z - far_z) % n_z) * 2 + (core + cc) % 2}

    def took(ref, sem):
        pltpu.make_async_copy(ref, ref, sem).wait()

    def dispatch(m):
        pltpu.make_async_remote_copy(
            src_ref=outbox.at[m],
            dst_ref=rows_in.at[0, m],
            send_sem=sent.at[0],
            recv_sem=z_recv.at[m // 4],
            device_id=expert_at(m),
            device_id_type=MESH,
        ).start()

    def give_back(m):
        pltpu.make_async_remote_copy(
            src_ref=summed.at[m],
            dst_ref=returned.at[m],
            send_sem=sent.at[1],
            recv_sem=b_recv.at[m // 4],
            device_id=source_at(m),
            device_id_type=MESH,
        ).start()

    def order(t):
        return (t + steps - 1) % steps

    def send_out(k, carry):
        m = (k + n_sp - 4) % n_sp

        @pl.when(m > 0)
        def _():
            dispatch(m)

        return carry

    pltpu.make_async_copy(outbox.at[0], rows_in.at[0, 0], z_recv.at[0]).start()
    lax.fori_loop(0, n_sp, send_out, 0)

    def side(to, src, dst, send, recv):
        pltpu.make_async_remote_copy(
            src_ref=src,
            dst_ref=dst,
            send_sem=sent.at[send],
            recv_sem=recv,
            device_id={"tp": to},
            device_id_type=MESH,
        ).start()

    for k in range(2):
        padded = jnp.concatenate(
            [gather[k], jnp.zeros((-n_rows % LANES, tokens), F32)], axis=0
        )
        pick[k * tokens : (k + 1) * tokens, :] = padded.T.astype(BF16)[:, :n_rows]

    def arrive(t):
        four = pl.ds(4 * t, 4)
        took(rows_in.at[0, four], z_recv.at[t])
        side(right, rows_in.at[0, four], rows_in.at[1, four], 2, g_recv.at[t])
        side(left, rows_in.at[0, four], rows_in.at[3, four], 2, g_recv.at[t])

    def forward(t):
        a, b = pl.ds(4 * t, 2), pl.ds(4 * t + 2, 2)
        took(rows_in.at[pl.ds(0, 2), pl.ds(4 * t, 4)], g_recv.at[t])
        side(right, rows_in.at[1, a], rows_in.at[2, a], 3, f_recv.at[t])
        side(left, rows_in.at[3, b], rows_in.at[2, b], 3, f_recv.at[t])

    m_in = 4 * n_tp
    main_in = m_in * ROWS

    def experts(t):
        four = pl.ds(4 * t, 4)
        took(rows_in.at[2, four], f_recv.at[t])
        for q in range(n_tp):
            tail[q * 4 * chunks : (q + 1) * 4 * chunks, :] = (
                rows_in[q, four, chunks * ROWS :, :].astype(F32).reshape(4 * chunks, LANES)
            )
        for c in range(0, chunks, 2):
            block = rows_in[:, four, c * ROWS : (c + 2) * ROWS, :].astype(F32)
            block = block.reshape(m_in, 2 * ROWS, LANES)
            for k in range(2):
                main = block[:, k * ROWS : (k + 1) * ROWS, :].reshape(main_in, LANES)
                last = tail[pl.ds(c + k, m_in, stride=chunks), :]
                x_rows[:, (c + k) * LANES : (c + k + 1) * LANES] = jnp.concatenate(
                    [main, last], axis=0
                ).astype(BF16)
        half = 256
        for c in range(0, hidden, half):
            cols = slice(c, c + half)
            gate = dot(x_rows[...], gate_w[:, cols])
            up = dot(x_rows[...], up_w[:, cols])
            gate = jnp.minimum(gate, 7.0)
            up = jnp.clip(up, -7.0, 7.0)
            act[:, cols] = (gate * jax.nn.sigmoid(1.702 * gate) * (up + 1.0)).astype(BF16)
        for c in range(0, chunks, 2):
            rows = dot(act[...], down_w[:, c * LANES : (c + 2) * LANES])

            def store(c, block):
                parts_out[:, four, c * ROWS : (c + 2) * ROWS, :] = block.reshape(
                    n_tp, 4, 2 * ROWS, LANES
                )

            pack_main(store, rows, c, m_in)
            for k in range(2):
                tail[pl.ds(c + k, m_in, stride=chunks), :] = rows[
                    main_in:, k * LANES : (k + 1) * LANES
                ]
        for q in range(n_tp):
            parts_out[q, four, chunks * ROWS :, :] = (
                tail[q * 4 * chunks : (q + 1) * 4 * chunks, :]
                .reshape(4, chunks, LANES)
                .astype(BF16)
            )
        a, b = pl.ds(4 * t, 2), pl.ds(4 * t + 2, 2)
        side(right, parts_out.at[2, a], relay.at[t, pl.ds(0, 2)], 4, p_recv.at[t])
        side(left, parts_out.at[2, b], relay.at[t, pl.ds(2, 2)], 4, p_recv.at[t])
        side(right, parts_out.at[3, b], sides.at[0, b], 5, s_recv.at[t])
        side(left, parts_out.at[1, a], sides.at[1, a], 5, s_recv.at[t])

    def add_relay(t):
        a, b = pl.ds(4 * t, 2), pl.ds(4 * t + 2, 2)
        took(relay.at[t], p_recv.at[t])
        parts_out[3, a] = (parts_out[3, a].astype(F32) + relay[t, 0:2].astype(F32)).astype(BF16)
        parts_out[1, b] = (parts_out[1, b].astype(F32) + relay[t, 2:4].astype(F32)).astype(BF16)
        side(right, parts_out.at[3, a], sides.at[0, a], 6, s_recv.at[t])
        side(left, parts_out.at[1, b], sides.at[1, b], 6, s_recv.at[t])

    def finish(t):
        four = pl.ds(4 * t, 4)
        took(sides.at[:, four], s_recv.at[t])
        total = sides[0, four].astype(F32) + sides[1, four].astype(F32)
        summed[four] = (total + parts_out[0, four].astype(F32)).astype(BF16)

        def back(j, carry):
            give_back(4 * t + j)
            return carry

        lax.fori_loop((t == 0).astype(jnp.int32), 4, back, 0)

        @pl.when(t == 0)
        def _():
            pltpu.make_async_copy(summed.at[0], returned.at[0], b_recv.at[0]).start()

    stages = (finish, add_relay, experts, forward, arrive)

    def pipeline(s, carry):
        for k, stage in enumerate(stages):
            t = s - (len(stages) - 1 - k)
            if stage is experts:

                @pl.when(t == 0)
                def _():
                    for load in loads[5:8]:
                        load.wait()

            @pl.when((t >= 0) & (t < steps))
            def _():
                stage(order(t))

        return carry

    lax.fori_loop(0, steps + len(stages) - 1, pipeline, 0)

    for k in range(steps):
        t = order(k)
        four = slice(4 * t, 4 * t + 4)
        took(returned.at[pl.ds(4 * t, 4)], b_recv.at[t])
        tail[: 4 * chunks, :] = (
            returned[four, chunks * ROWS :, :].astype(F32).reshape(4 * chunks, LANES)
        )
        for c in range(0, chunks, 2):
            block = returned[four, c * ROWS : (c + 2) * ROWS, :].astype(F32)
            for k in range(2):
                main = block[:, k * ROWS : (k + 1) * ROWS, :].reshape(4 * ROWS, LANES)
                cols = slice((c + k) * LANES, (c + k + 1) * LANES)
                r_rows[4 * t * ROWS : 4 * (t + 1) * ROWS, cols] = main.astype(BF16)
                r_last[4 * t : 4 * t + 4, cols] = tail[pl.ds(c + k, 4, stride=chunks), :]

    def out_copy(c):
        cols = pl.ds(c, tile)
        return pltpu.make_async_copy(out_rows.at[:, cols], out_hbm.at[:, cols], sent.at[7])

    weights = jnp.concatenate([wts_ref[...], jnp.zeros((LANES - 2, tokens), F32)], axis=0).T
    square = jnp.zeros((tokens, LANES), F32)
    for c in range(0, width, tile):
        cols = slice(c, c + tile)
        two = dot(pick[:, :n_main], r_rows[:, cols]) + dot(
            pick[:, n_main:], r_last[:, cols].astype(BF16)
        )
        moe = two[:tokens] * weights[:, 0:1] + two[tokens:] * weights[:, 1:2]
        wide[:, cols] = moe
        square = square + fold(moe * moe)
    scale = lax.rsqrt(jnp.sum(square, axis=1, keepdims=True) * (1.0 / width) + EPS)
    for c in range(0, width, tile):
        cols = slice(c, c + tile)
        out_rows[:, cols] = (
            stream[:, cols].astype(F32) + wide[:, cols] * scale * post_exp_ref[:, cols]
        ).astype(BF16)
        out_copy(c).start()

    for halo in halos:
        halo.wait_send()
    took(outbox.at[pl.ds(1, n_sp - 1)], sent.at[0])
    took(summed.at[pl.ds(1, n_sp - 1)], sent.at[1])
    took(rows_in.at[pl.ds(0, 2)], sent.at[2])
    took(rows_in.at[0], sent.at[3])
    for k in range(4, 7):
        took(parts_out.at[0], sent.at[k])
    took(out_rows, sent.at[7])


def layer(
    n_sp,
    n_tp,
    residual_in,
    out_gate,
    in_gate,
    conv_input,
    conv_kernel,
    mix_out,
    post_mix_gain,
    pre_expert_gain,
    post_expert_gain,
    expert_ids,
    expert_weights,
    gate_proj,
    up_proj,
    down_proj,
):
    tokens, width = residual_in.shape
    conv_w = in_gate.shape[1]
    hidden = gate_proj.shape[2]
    chunks = width // LANES
    steps = n_sp // 4
    msg = (ROWS + 1) * chunks
    n_main = n_sp * ROWS
    rows_step = 4 * n_tp * (ROWS + 1)
    anyspace = pl.BlockSpec(memory_space=pl.ANY)
    dma = pltpu.SemaphoreType.DMA
    scratch = [
        pltpu.VMEM((2, tokens), jnp.int32),
        pltpu.VMEM((2, tokens), F32),
        pltpu.VMEM(conv_kernel.shape, BF16),
        pltpu.VMEM((1, width), F32),
        pltpu.VMEM((1, width), F32),
        pltpu.VMEM((1, width), F32),
        pltpu.VMEM((tokens, conv_w), BF16),
        pltpu.VMEM((tokens, conv_w), BF16),
        pltpu.VMEM((tokens, conv_w), BF16),
        pltpu.VMEM((tokens, width), BF16),
        pltpu.VMEM((conv_w, width), BF16),
        pltpu.VMEM((width, hidden), BF16),
        pltpu.VMEM((width, hidden), BF16),
        pltpu.VMEM((hidden, width), BF16),
        pltpu.VMEM((2, conv_w), BF16),
        pltpu.VMEM((2, conv_w), BF16),
        pltpu.VMEM((2, conv_w), BF16),
        pltpu.VMEM((2, conv_w), BF16),
        pltpu.VMEM((tokens, conv_w), BF16),
        pltpu.VMEM((tokens, width), F32),
        pltpu.VMEM((tokens, width), BF16),
        pltpu.VMEM((tokens, width), BF16),
        pltpu.VMEM((2 * tokens, n_main + n_sp), BF16),
        pltpu.VMEM((n_sp, msg, LANES), BF16),
        pltpu.VMEM((n_tp, n_sp, msg, LANES), BF16),
        pltpu.VMEM((n_tp, n_sp, msg, LANES), BF16),
        pltpu.VMEM((steps, 4, msg, LANES), BF16),
        pltpu.VMEM((2, n_sp, msg, LANES), BF16),
        pltpu.VMEM((n_sp, msg, LANES), BF16),
        pltpu.VMEM((n_sp, msg, LANES), BF16),
        pltpu.VMEM((n_sp * chunks, LANES), F32),
        pltpu.VMEM((rows_step, width), BF16),
        pltpu.VMEM((rows_step, hidden), BF16),
        pltpu.VMEM((n_main, width), BF16),
        pltpu.VMEM((n_sp, width), F32),
        pltpu.VMEM((tokens, width), BF16),
        dma((14,)),
        dma((2,)),
        dma((2,)),
    ]
    scratch += [dma((steps,)) for _ in range(6)]
    scratch += [dma((8,))]
    return pl.pallas_call(
        functools.partial(layer_kernel, n_sp, n_tp),
        out_shape=jax.ShapeDtypeStruct((tokens, width), BF16),
        in_specs=[anyspace] * 14,
        out_specs=anyspace,
        scratch_shapes=scratch,
        compiler_params=pltpu.CompilerParams(
            collective_id=0, has_side_effects=True, vmem_limit_bytes=62 * 1024 * 1024
        ),
    )(
        expert_ids.T,
        expert_weights.T,
        conv_kernel,
        post_mix_gain.reshape(1, width),
        pre_expert_gain.reshape(1, width),
        post_expert_gain.reshape(1, width),
        in_gate,
        conv_input,
        out_gate,
        residual_in,
        mix_out,
        gate_proj[0],
        up_proj[0],
        down_proj[0],
    )


def solution(mesh):
    tok = P(TOKENS_OVER, None)
    in_specs = (tok, tok, tok, tok, P(), P(), P(), P(), P(), tok, tok)
    in_specs += (P("sp", None, "tp"), P("sp", None, "tp"), P("sp", "tp", None))
    return jax.shard_map(
        functools.partial(layer, mesh.shape["sp"], mesh.shape["tp"]),
        mesh=mesh,
        in_specs=in_specs,
        out_specs=tok,
        check_vma=False,
    )
```

```python
import functools

import jax
import jax.numpy as jnp
from jax import lax
from jax.experimental import pallas as pl
from jax.experimental.pallas import tpu as pltpu
from jax.sharding import PartitionSpec as P

TOKENS_OVER = ("grp", "sp", "tp")
MESH = pl.DeviceIdType.MESH
F32 = jnp.float32
BF16 = jnp.bfloat16
LANES = 128
ROWS = 8
EPS = 1e-06


def dot(a, b):
    return jnp.dot(a, b, preferred_element_type=F32)


def layer_kernel(
    n_sp,
    n_tp,
    ids_hbm,
    wts_hbm,
    taps_hbm,
    post_mix_hbm,
    pre_exp_hbm,
    post_exp_hbm,
    in_gate_hbm,
    conv_in_hbm,
    out_gate_hbm,
    resid_hbm,
    mix_hbm,
    gate_hbm,
    up_hbm,
    down_hbm,
    out_hbm,
    ids_ref,
    wts_ref,
    taps_ref,
    post_mix_ref,
    pre_exp_ref,
    post_exp_ref,
    in_gate,
    conv_in,
    out_gate,
    resid,
    mix_w,
    gate_w,
    up_w,
    down_w,
    edge_g,
    edge_c,
    halo_g,
    halo_c,
    mixed,
    wide,
    stream,
    normed,
    pick,
    outbox,
    rows_in,
    parts_out,
    relay,
    sides,
    summed,
    returned,
    tail,
    x_rows,
    act,
    r_rows,
    r_last,
    out_rows,
    load_sem,
    halo_send,
    halo_recv,
    z_recv,
    g_recv,
    f_recv,
    p_recv,
    s_recv,
    b_recv,
    sent,
):
    tokens, width = resid.shape
    conv_w = in_gate.shape[1]
    hidden = gate_w.shape[1]
    chunks = width // LANES
    n_z = n_sp // 2
    steps = n_z // 2
    n_main = n_sp * ROWS
    n_rows = n_main + n_sp
    me = lax.axis_index("sp")
    z, core = me // 2, me % 2
    x = lax.axis_index("tp")
    right = (x + 1) % n_tp
    left = (x + n_tp - 1) % n_tp
    place = me * n_tp + x
    after = (place + 1) % (n_sp * n_tp)
    before = (place + n_sp * n_tp - 1) % (n_sp * n_tp)

    def device_at(p):
        return {"sp": p // n_tp, "tp": p % n_tp}

    bar = pltpu.get_barrier_semaphore()

    def enter(who):
        pl.semaphore_signal(bar, inc=1, device_id=who, device_id_type=MESH)

    def greet(k, carry):
        far_up = steps - (k + 1) // 2
        up = far_up + (k % 2) * (n_z - 2 * far_up)
        for c in range(2):
            enter({"sp": ((z + up) % n_z) * 2 + c})
        return carry

    lax.fori_loop(0, n_z - 1, greet, 0)
    for who in ({"sp": me + 1 - 2 * core}, device_at(after), device_at(before)):
        enter(who)
    for who in ({"tp": right}, {"tp": left}):
        enter(who)

    loads = [
        pltpu.make_async_copy(src, dst, load_sem.at[k])
        for k, (src, dst) in enumerate(
            (
                (in_gate_hbm, in_gate),
                (conv_in_hbm, conv_in),
                (out_gate_hbm, out_gate),
                (mix_hbm, mix_w),
                (resid_hbm, resid),
                (gate_hbm, gate_w),
                (up_hbm, up_w),
                (down_hbm, down_w),
                (ids_hbm, ids_ref),
                (taps_hbm, taps_ref),
                (post_mix_hbm, post_mix_ref),
                (pre_exp_hbm, pre_exp_ref),
                (wts_hbm, wts_ref),
                (post_exp_hbm, post_exp_ref),
            )
        )
    ]
    for load in loads[:2] + loads[8:10] + loads[2:5] + loads[10:] + loads[5:8]:
        load.start()
    loads[8].wait()

    ids = ids_ref[...]
    e_z, e_core = ids // 2, ids % 2
    dz = (e_z - z + n_z) % n_z
    far = dz >= steps
    step_of = jnp.where(far, dz - steps, (steps - dz) % steps)
    message = step_of * 4 + jnp.where(far, 2, 0) + (e_core + core) % 2
    place_iota = lax.broadcasted_iota(jnp.int32, (n_sp, tokens), 0)
    hot = [(place_iota == message[k : k + 1, :]) for k in range(2)]
    both = hot[0].astype(F32) + hot[1].astype(F32)
    earlier = (
        lax.broadcasted_iota(jnp.int32, (tokens, tokens), 0)
        < lax.broadcasted_iota(jnp.int32, (tokens, tokens), 1)
    ).astype(F32)
    count = dot(both.astype(BF16), earlier.astype(BF16))
    row_iota = lax.broadcasted_iota(jnp.int32, (n_rows, tokens), 0)
    gather = []
    for k in range(2):
        slot = jnp.sum(jnp.where(hot[k], count, 0.0), axis=0, keepdims=True).astype(jnp.int32)
        msg = message[k : k + 1, :]
        code = jnp.where(slot < ROWS, msg * ROWS + slot, n_main + msg)
        gather.append((row_iota == code).astype(F32))
    spread = (gather[0] + gather[1]).astype(BF16)

    for load, src, edge in ((loads[0], in_gate, edge_g), (loads[1], conv_in, edge_c)):
        load.wait()
        edge[...] = src[tokens - 2 :, :]

    head_rows = 16
    inside = (place > 0).astype(F32)
    loads[9].wait()
    taps = taps_ref[...].astype(F32)

    def convolve(rows, with_halo):
        row_of = lax.broadcasted_iota(jnp.int32, (rows, 1), 0)
        col = 256
        for c in range(0, conv_w, col):
            cols = slice(c, c + col)
            u = in_gate[:rows, cols].astype(F32) * conv_in[:rows, cols].astype(F32)
            one, two = pltpu.roll(u, 1, 0), pltpu.roll(u, 2, 0)
            if with_halo:
                head = halo_g[:, cols].astype(F32) * halo_c[:, cols].astype(F32) * inside
                one = jnp.where(row_of == 0, head[1:2], one)
                two = jnp.where(row_of == 1, head[1:2], two)
                two = jnp.where(row_of == 0, head[0:1], two)
            conv = taps[0:1, cols] * two + taps[1:2, cols] * one + taps[2:3, cols] * u
            mixed[:rows, cols] = (out_gate[:rows, cols].astype(F32) * conv).astype(BF16)

    loads[2].wait()
    convolve(tokens, False)
    pl.semaphore_wait(bar, n_sp - 1 + 4)

    halos = [
        pltpu.make_async_remote_copy(
            src_ref=src,
            dst_ref=dst,
            send_sem=halo_send.at[k],
            recv_sem=halo_recv.at[k],
            device_id=device_at(after),
            device_id_type=MESH,
        )
        for k, (src, dst) in enumerate(((edge_g, halo_g), (edge_c, halo_c)))
    ]
    for halo in halos:
        halo.start()
    for load in loads[3:5] + loads[10:]:
        load.wait()
    for halo in halos:
        halo.wait_recv()
    convolve(head_rows, True)

    tile = 512
    square = jnp.zeros((tokens, LANES), F32)

    def fold(v):
        total = v[:, :LANES]
        for k in range(LANES, v.shape[1], LANES):
            total = total + v[:, k : k + LANES]
        return total

    for c in range(0, width, tile):
        cols = slice(c, c + tile)
        proj = dot(mixed[...], mix_w[:, cols])
        wide[:, cols] = proj
        square = square + fold(proj * proj)
    scale = lax.rsqrt(jnp.sum(square, axis=1, keepdims=True) * (1.0 / width) + EPS)
    square = jnp.zeros((tokens, LANES), F32)
    for c in range(0, width, tile):
        cols = slice(c, c + tile)
        s = resid[:, cols].astype(F32) + wide[:, cols] * scale * post_mix_ref[:, cols]
        s = s.astype(BF16)
        stream[:, cols] = s
        s = s.astype(F32)
        square = square + fold(s * s)
    scale = lax.rsqrt(jnp.sum(square, axis=1, keepdims=True) * (1.0 / width) + EPS)
    for c in range(0, width, tile):
        cols = slice(c, c + tile)
        normed[:, cols] = (stream[:, cols].astype(F32) * scale * pre_exp_ref[:, cols]).astype(BF16)

    def pack_main(store, rows, c, count_of):
        pair = [
            rows[: count_of * ROWS, k * LANES : (k + 1) * LANES].reshape(count_of, ROWS, LANES)
            for k in range(2)
        ]
        store(c, jnp.concatenate(pair, axis=1).astype(BF16))

    for c in range(0, chunks, 2):
        rows = dot(spread, normed[:, c * LANES : (c + 2) * LANES])

        def store(c, block):
            outbox[:, c * ROWS : (c + 2) * ROWS, :] = block

        pack_main(store, rows, c, n_sp)
        for k in range(2):
            tail[pl.ds(c + k, n_sp, stride=chunks), :] = rows[
                n_main:, k * LANES : (k + 1) * LANES
            ]
    outbox[:, chunks * ROWS :, :] = tail[...].reshape(n_sp, chunks, LANES).astype(BF16)

    def expert_at(m):
        step, half, cc = m // 4, (m // 2) % 2, m % 2
        far_z = (1 - half) * ((steps - step) % steps) + half * (steps + step)
        return {"sp": ((z + far_z) % n_z) * 2 + (core + cc) % 2}

    def source_at(m):
        step, half, cc = m // 4, (m // 2) % 2, m % 2
        far_z = (1 - half) * ((steps - step) % steps) + half * (steps + step)
        return {"sp": ((z + n_z - far_z) % n_z) * 2 + (core + cc) % 2}

    def took(ref, sem):
        pltpu.make_async_copy(ref, ref, sem).wait()

    def dispatch(m):
        pltpu.make_async_remote_copy(
            src_ref=outbox.at[m],
            dst_ref=rows_in.at[0, m],
            send_sem=sent.at[0],
            recv_sem=z_recv.at[m // 4],
            device_id=expert_at(m),
            device_id_type=MESH,
        ).start()

    def give_back(m):
        pltpu.make_async_remote_copy(
            src_ref=summed.at[m],
            dst_ref=returned.at[m],
            send_sem=sent.at[1],
            recv_sem=b_recv.at[m // 4],
            device_id=source_at(m),
            device_id_type=MESH,
        ).start()

    def order(t):
        return (t + steps - 1) % steps

    pltpu.make_async_copy(outbox.at[0], rows_in.at[0, 0], z_recv.at[0]).start()
    for k in range(n_sp):
        if (k + n_sp - 4) % n_sp > 0:
            dispatch((k + n_sp - 4) % n_sp)

    def side(to, src, dst, send, recv):
        pltpu.make_async_remote_copy(
            src_ref=src,
            dst_ref=dst,
            send_sem=sent.at[send],
            recv_sem=recv,
            device_id={"tp": to},
            device_id_type=MESH,
        ).start()

    for k in range(2):
        padded = jnp.concatenate(
            [gather[k], jnp.zeros((-n_rows % LANES, tokens), F32)], axis=0
        )
        pick[k * tokens : (k + 1) * tokens, :] = padded.T.astype(BF16)[:, :n_rows]

    def arrive(t):
        four = pl.ds(4 * t, 4)
        took(rows_in.at[0, four], z_recv.at[t])
        side(right, rows_in.at[0, four], rows_in.at[1, four], 2, g_recv.at[t])
        side(left, rows_in.at[0, four], rows_in.at[3, four], 2, g_recv.at[t])

    def forward(t):
        a, b = pl.ds(4 * t, 2), pl.ds(4 * t + 2, 2)
        took(rows_in.at[pl.ds(0, 2), pl.ds(4 * t, 4)], g_recv.at[t])
        side(right, rows_in.at[1, a], rows_in.at[2, a], 3, f_recv.at[t])
        side(left, rows_in.at[3, b], rows_in.at[2, b], 3, f_recv.at[t])

    m_in = 4 * n_tp
    main_in = m_in * ROWS

    def experts(t):
        four = pl.ds(4 * t, 4)
        took(rows_in.at[2, four], f_recv.at[t])
        for q in range(n_tp):
            tail[q * 4 * chunks : (q + 1) * 4 * chunks, :] = (
                rows_in[q, four, chunks * ROWS :, :].astype(F32).reshape(4 * chunks, LANES)
            )
        for c in range(0, chunks, 2):
            block = rows_in[:, four, c * ROWS : (c + 2) * ROWS, :].astype(F32)
            block = block.reshape(m_in, 2 * ROWS, LANES)
            for k in range(2):
                main = block[:, k * ROWS : (k + 1) * ROWS, :].reshape(main_in, LANES)
                last = tail[pl.ds(c + k, m_in, stride=chunks), :]
                x_rows[:, (c + k) * LANES : (c + k + 1) * LANES] = jnp.concatenate(
                    [main, last], axis=0
                ).astype(BF16)
        half = 256
        for c in range(0, hidden, half):
            cols = slice(c, c + half)
            gate = dot(x_rows[...], gate_w[:, cols])
            up = dot(x_rows[...], up_w[:, cols])
            gate = jnp.minimum(gate, 7.0)
            up = jnp.clip(up, -7.0, 7.0)
            act[:, cols] = (gate * jax.nn.sigmoid(1.702 * gate) * (up + 1.0)).astype(BF16)
        for c in range(0, chunks, 2):
            rows = dot(act[...], down_w[:, c * LANES : (c + 2) * LANES])

            def store(c, block):
                parts_out[:, four, c * ROWS : (c + 2) * ROWS, :] = block.reshape(
                    n_tp, 4, 2 * ROWS, LANES
                )

            pack_main(store, rows, c, m_in)
            for k in range(2):
                tail[pl.ds(c + k, m_in, stride=chunks), :] = rows[
                    main_in:, k * LANES : (k + 1) * LANES
                ]
        for q in range(n_tp):
            parts_out[q, four, chunks * ROWS :, :] = (
                tail[q * 4 * chunks : (q + 1) * 4 * chunks, :]
                .reshape(4, chunks, LANES)
                .astype(BF16)
            )
        a, b = pl.ds(4 * t, 2), pl.ds(4 * t + 2, 2)
        side(right, parts_out.at[2, a], relay.at[t, pl.ds(0, 2)], 4, p_recv.at[t])
        side(left, parts_out.at[2, b], relay.at[t, pl.ds(2, 2)], 4, p_recv.at[t])
        side(right, parts_out.at[3, b], sides.at[0, b], 5, s_recv.at[t])
        side(left, parts_out.at[1, a], sides.at[1, a], 5, s_recv.at[t])

    def add_relay(t):
        a, b = pl.ds(4 * t, 2), pl.ds(4 * t + 2, 2)
        took(relay.at[t], p_recv.at[t])
        parts_out[3, a] = (parts_out[3, a].astype(F32) + relay[t, 0:2].astype(F32)).astype(BF16)
        parts_out[1, b] = (parts_out[1, b].astype(F32) + relay[t, 2:4].astype(F32)).astype(BF16)
        side(right, parts_out.at[3, a], sides.at[0, a], 6, s_recv.at[t])
        side(left, parts_out.at[1, b], sides.at[1, b], 6, s_recv.at[t])

    def finish(t):
        four = pl.ds(4 * t, 4)
        took(sides.at[:, four], s_recv.at[t])
        total = sides[0, four].astype(F32) + sides[1, four].astype(F32)
        summed[four] = (total + parts_out[0, four].astype(F32)).astype(BF16)

        def back(j, carry):
            give_back(4 * t + j)
            return carry

        lax.fori_loop((t == 0).astype(jnp.int32), 4, back, 0)

        @pl.when(t == 0)
        def _():
            pltpu.make_async_copy(summed.at[0], returned.at[0], b_recv.at[0]).start()

    stages = (finish, add_relay, experts, forward, arrive)

    def pipeline(s, carry):
        for k, stage in enumerate(stages):
            t = s - (len(stages) - 1 - k)
            if stage is experts:

                @pl.when(t == 0)
                def _():
                    for load in loads[5:8]:
                        load.wait()

            @pl.when((t >= 0) & (t < steps))
            def _():
                stage(order(t))

        return carry

    lax.fori_loop(0, steps + len(stages) - 1, pipeline, 0)

    for k in range(steps):
        t = order(k)
        four = slice(4 * t, 4 * t + 4)
        took(returned.at[pl.ds(4 * t, 4)], b_recv.at[t])
        tail[: 4 * chunks, :] = (
            returned[four, chunks * ROWS :, :].astype(F32).reshape(4 * chunks, LANES)
        )
        for c in range(0, chunks, 2):
            block = returned[four, c * ROWS : (c + 2) * ROWS, :].astype(F32)
            for k in range(2):
                main = block[:, k * ROWS : (k + 1) * ROWS, :].reshape(4 * ROWS, LANES)
                cols = slice((c + k) * LANES, (c + k + 1) * LANES)
                r_rows[4 * t * ROWS : 4 * (t + 1) * ROWS, cols] = main.astype(BF16)
                r_last[4 * t : 4 * t + 4, cols] = tail[pl.ds(c + k, 4, stride=chunks), :]

    def out_copy(c):
        cols = pl.ds(c, tile)
        return pltpu.make_async_copy(out_rows.at[:, cols], out_hbm.at[:, cols], sent.at[7])

    weights = jnp.concatenate([wts_ref[...], jnp.zeros((LANES - 2, tokens), F32)], axis=0).T
    square = jnp.zeros((tokens, LANES), F32)
    for c in range(0, width, tile):
        cols = slice(c, c + tile)
        two = dot(pick[:, :n_main], r_rows[:, cols]) + dot(
            pick[:, n_main:], r_last[:, cols].astype(BF16)
        )
        moe = two[:tokens] * weights[:, 0:1] + two[tokens:] * weights[:, 1:2]
        wide[:, cols] = moe
        square = square + fold(moe * moe)
    scale = lax.rsqrt(jnp.sum(square, axis=1, keepdims=True) * (1.0 / width) + EPS)
    for c in range(0, width, tile):
        cols = slice(c, c + tile)
        out_rows[:, cols] = (
            stream[:, cols].astype(F32) + wide[:, cols] * scale * post_exp_ref[:, cols]
        ).astype(BF16)
        out_copy(c).start()

    for halo in halos:
        halo.wait_send()
    took(outbox.at[pl.ds(1, n_sp - 1)], sent.at[0])
    took(summed.at[pl.ds(1, n_sp - 1)], sent.at[1])
    took(rows_in.at[pl.ds(0, 2)], sent.at[2])
    took(rows_in.at[0], sent.at[3])
    for k in range(4, 7):
        took(parts_out.at[0], sent.at[k])
    took(out_rows, sent.at[7])


def layer(
    n_sp,
    n_tp,
    residual_in,
    out_gate,
    in_gate,
    conv_input,
    conv_kernel,
    mix_out,
    post_mix_gain,
    pre_expert_gain,
    post_expert_gain,
    expert_ids,
    expert_weights,
    gate_proj,
    up_proj,
    down_proj,
):
    tokens, width = residual_in.shape
    conv_w = in_gate.shape[1]
    hidden = gate_proj.shape[2]
    chunks = width // LANES
    steps = n_sp // 4
    msg = (ROWS + 1) * chunks
    n_main = n_sp * ROWS
    rows_step = 4 * n_tp * (ROWS + 1)
    anyspace = pl.BlockSpec(memory_space=pl.ANY)
    dma = pltpu.SemaphoreType.DMA
    scratch = [
        pltpu.VMEM((2, tokens), jnp.int32),
        pltpu.VMEM((2, tokens), F32),
        pltpu.VMEM(conv_kernel.shape, BF16),
        pltpu.VMEM((1, width), F32),
        pltpu.VMEM((1, width), F32),
        pltpu.VMEM((1, width), F32),
        pltpu.VMEM((tokens, conv_w), BF16),
        pltpu.VMEM((tokens, conv_w), BF16),
        pltpu.VMEM((tokens, conv_w), BF16),
        pltpu.VMEM((tokens, width), BF16),
        pltpu.VMEM((conv_w, width), BF16),
        pltpu.VMEM((width, hidden), BF16),
        pltpu.VMEM((width, hidden), BF16),
        pltpu.VMEM((hidden, width), BF16),
        pltpu.VMEM((2, conv_w), BF16),
        pltpu.VMEM((2, conv_w), BF16),
        pltpu.VMEM((2, conv_w), BF16),
        pltpu.VMEM((2, conv_w), BF16),
        pltpu.VMEM((tokens, conv_w), BF16),
        pltpu.VMEM((tokens, width), F32),
        pltpu.VMEM((tokens, width), BF16),
        pltpu.VMEM((tokens, width), BF16),
        pltpu.VMEM((2 * tokens, n_main + n_sp), BF16),
        pltpu.VMEM((n_sp, msg, LANES), BF16),
        pltpu.VMEM((n_tp, n_sp, msg, LANES), BF16),
        pltpu.VMEM((n_tp, n_sp, msg, LANES), BF16),
        pltpu.VMEM((steps, 4, msg, LANES), BF16),
        pltpu.VMEM((2, n_sp, msg, LANES), BF16),
        pltpu.VMEM((n_sp, msg, LANES), BF16),
        pltpu.VMEM((n_sp, msg, LANES), BF16),
        pltpu.VMEM((n_sp * chunks, LANES), F32),
        pltpu.VMEM((rows_step, width), BF16),
        pltpu.VMEM((rows_step, hidden), BF16),
        pltpu.VMEM((n_main, width), BF16),
        pltpu.VMEM((n_sp, width), F32),
        pltpu.VMEM((tokens, width), BF16),
        dma((14,)),
        dma((2,)),
        dma((2,)),
    ]
    scratch += [dma((steps,)) for _ in range(6)]
    scratch += [dma((8,))]
    return pl.pallas_call(
        functools.partial(layer_kernel, n_sp, n_tp),
        out_shape=jax.ShapeDtypeStruct((tokens, width), BF16),
        in_specs=[anyspace] * 14,
        out_specs=anyspace,
        scratch_shapes=scratch,
        compiler_params=pltpu.CompilerParams(
            collective_id=0, has_side_effects=True, vmem_limit_bytes=62 * 1024 * 1024
        ),
    )(
        expert_ids.T,
        expert_weights.T,
        conv_kernel,
        post_mix_gain.reshape(1, width),
        pre_expert_gain.reshape(1, width),
        post_expert_gain.reshape(1, width),
        in_gate,
        conv_input,
        out_gate,
        residual_in,
        mix_out,
        gate_proj[0],
        up_proj[0],
        down_proj[0],
    )


def solution(mesh):
    tok = P(TOKENS_OVER, None)
    in_specs = (tok, tok, tok, tok, P(), P(), P(), P(), P(), tok, tok)
    in_specs += (P("sp", None, "tp"), P("sp", None, "tp"), P("sp", "tp", None))
    return jax.shard_map(
        functools.partial(layer, mesh.shape["sp"], mesh.shape["tp"]),
        mesh=mesh,
        in_specs=in_specs,
        out_specs=tok,
        check_vma=False,
    )
```
